128 devices in a mesh: sp: 64 (over z, y, x), tp: 2 (over core).
Axes of the slice: x: 4, y: 4, z: 4, core: 2. Of those that a mesh axis runs over, the one named last changes fastest.
Arguments:
- wide_inputs: bfloat16 [8192, 512], P('sp', 'tp'), may hold values from -6 to 6
- narrow_inputs: bfloat16 [8192, 512], P('sp', 'tp'), may hold values from -6 to 6
- wide_poles: float32 [2, 2, 32, 64], P(None, None, 'tp'), may hold values from -3.1416 to 3.1416, as said below
- narrow_poles: float32 [2, 2, 32, 32], P(None, None, 'tp'), may hold values from -3.1416 to 3.1416, as said below
- step_sizes: float32 [2, 2, 32], P(None, None, 'tp'), may hold values from 0 to 1, as said below
- forget: float32 [2, 2, 32, 8192], P(None, None, 'tp', 'sp'), may hold values from 0 to 2.2
- wide_in_map: float32 [2, 2, 32, 16, 64], P(None, None, 'tp'), may hold values from -2.5 to 2.5
- narrow_in_map: float32 [2, 2, 32, 16, 32], P(None, None, 'tp'), may hold values from -2.5 to 2.5
- wide_out_map: float32 [2, 2, 32, 16, 64], P(None, None, 'tp'), may hold values from -1.25 to 1.25
- narrow_out_map: float32 [2, 2, 32, 16, 32], P(None, None, 'tp'), may hold values from -2 to 2
- skip_weight: bfloat16 [2, 512], P(None, 'tp'), may hold values from -6 to 6
- gate_mix: bfloat16 [2, 32, 16, 16], P(None, 'tp'), may hold values from -1.5 to 1.5
- residual: bfloat16 [8192, 2048], P(('sp', 'tp')), may hold values from -6 to 6
- mixer_gain: float32 [1024], replicated, may hold values from 0.1 to 1.9
- out_proj: bfloat16 [1024, 2048], replicated, may hold values from -0.1875 to 0.1875
- ffn_gain: float32 [2048], replicated, may hold values from 0.1 to 1.9
- routes: int32 [8192, 2], P(('sp', 'tp')), may hold values from 0 to 127, all different within a row; in each aligned block of 64 rows (0 to 63, 64 to 127, ...) at most 2 rows name the same one
- route_weights: float32 [8192, 2], P(('sp', 'tp')), may hold values from 0.1 to 1
- gate_proj: bfloat16 [128, 2048, 1408], P(('sp', 'tp')), may hold values from -0.125 to 0.125
- up_proj: bfloat16 [128, 2048, 1408], P(('sp', 'tp')), may hold values from -0.125 to 0.125
- down_proj: bfloat16 [128, 1408, 2048], P(('sp', 'tp')), may hold values from -0.15625 to 0.15625
Outputs:
- layer_out: bfloat16 [8192, 2048], P(('sp', 'tp'))
The draws below stay inside these ranges and needn't reach their ends.
Inputs may be any that keep to these rules, and one draw needn't show every extreme that they name: `routes`: in each aligned block of 64 rows (the rows of one device), no expert is named by more than 2 entries, and the 2 experts of a row differ. `wide_poles`: along dimension 1, entry 0 (the real part) is negative and entry 1 (the imaginary part) is at least 0.1 in magnitude. `narrow_poles`: along dimension 1, entry 0 (the real part) is negative and entry 1 (the imaginary part) is at least 0.1 in magnitude. `step_sizes`: Positive.
All inputs are finite; a program needn't handle non-finite values.
Results may differ from the reference program's by a relative error of at most 0.014.
Values may be sent and summed in bfloat16 or wider, within the bound.
A program may use at most 192 MiB of HBM per device.

```python
import math
import jax
import jax.numpy as jnp
import numpy as np
from jax import lax

D = 2048
GROUPS = 32
CHANNELS = 16
WIDE_STATE = 64
NARROW_STATE = 32
FE = 1408
TOP = 2
TOK_DEV = 128
TOKENS = 8192
ROWS = 64
SETW = 512
EXPERTS = 128
CAP = 2


def pick_slow(key):
    chance = 0.5
    return jax.random.bernoulli(jax.random.fold_in(key, 101), chance, (2, 2, GROUPS))


def make_poles(key, which, states):
    slow = pick_slow(key)[:, which]
    keys = jax.random.split(jax.random.fold_in(key, 11 + which), 4)
    slow_rate = jnp.exp(jax.random.uniform(keys[0], (2, GROUPS, states), jnp.float32, math.log(0.05), math.log(0.5))) / TOKENS
    fast_rate = jnp.exp(jax.random.uniform(keys[1], (2, GROUPS, states), jnp.float32, math.log(0.02), math.log(0.1)))
    decay_re = -jnp.where(slow[:, :, None], slow_rate, fast_rate)
    signs = jnp.where(jax.random.bernoulli(keys[3], 0.5, (2, GROUPS, states)), 1.0, -1.0)
    decay_im = jax.random.uniform(keys[2], (2, GROUPS, states), jnp.float32, 0.1, 3.14) * signs
    return jnp.stack([decay_re, decay_im], axis=1).astype(jnp.float32)


def draw_wide_poles(key, part):
    return make_poles(key, 0, WIDE_STATE)


def draw_narrow_poles(key, part):
    return make_poles(key, 1, NARROW_STATE)


def draw_step_sizes(key, part):
    slow = pick_slow(key)
    base = jnp.exp(jax.random.uniform(jax.random.fold_in(key, 21), (2, 2, GROUPS), jnp.float32, math.log(0.5), math.log(2.0)))
    return (base * jnp.where(slow, math.sqrt(0.4 / TOKENS), 0.3)).astype(jnp.float32)


def draw_forget(key, part):
    keys = jax.random.split(jax.random.fold_in(key, 31), 3)
    blocks = TOKENS // TOK_DEV
    factor = jnp.exp(jax.random.uniform(keys[0], (2, 2, GROUPS, blocks), jnp.float32, math.log(0.1), math.log(1.0)))
    decay_speed = jnp.repeat(factor, TOK_DEV, axis=3) / TOKENS
    spots = jax.random.randint(keys[1], (2, 2, GROUPS, 3), 0, TOKENS)
    total_quantity = jax.random.uniform(keys[2], (2, 2, GROUPS, 3), jnp.float32, 0.22, 0.69)
    slot_positions = jnp.arange(TOKENS)[None, None, None, None, :] == spots[:, :, :, :, None]
    signal_segments = jnp.sum(jnp.where(slot_positions, total_quantity[:, :, :, :, None], 0.0), axis=3)
    return (decay_speed + signal_segments).astype(jnp.float32)


def block_levels(stream_key, extent, cuts, least, top_value):
    factor_of = 1.0
    for position, parts in cuts:
        heights = jax.random.uniform(jax.random.fold_in(jax.random.fold_in(stream_key, 6), position), (parts,), jnp.float32, least / len(cuts), top_value / len(cuts))
        factor_of = factor_of * jnp.repeat(jnp.exp(heights), extent[position] // parts).reshape((-1,) + (1,) * (len(extent) - 1 - position))
    return factor_of


def assign_block(stream_key, own, number, rows, number_of, top, reach, skew):
    sequence = jax.random.permutation(stream_key, number_of)
    packed, common = shares(number_of, rows * top, reach, skew, True), shares(number_of, rows * top, reach, skew, False)
    places = jnp.arange(number_of)

    def named(tallies, rotation):
        used = int((tallies > 0).sum())
        fixed = max(1, used // 4)
        shifted = fixed + (places - fixed + rotation * (used - fixed)) % max(1, number_of - fixed)
        return jnp.zeros((number_of,), jnp.int32).at[sequence[jnp.where(places < fixed, places, shifted)]].set(jnp.asarray(tallies, jnp.int32))

    tallies = jnp.where(number % 4 == 0, named(packed, number // 4), named(common, number - number // 4 - 1))
    mixed = jax.random.permutation(jax.random.fold_in(own, 3), number_of)
    donor, sink = mixed[0:number_of // 2 * 2:2], mixed[1:number_of // 2 * 2:2]
    slack = jnp.minimum(tallies[donor] - 1, reach - tallies[sink]) // 2
    slack = jnp.where((donor == sequence[0]) | (sink == sequence[0]) | (tallies[sink] == 0), 0, jnp.maximum(slack, 0))
    shifted = jax.random.randint(jax.random.fold_in(own, 4), (number_of // 2,), 0, 1 << 20) % (slack + 1)
    tallies = tallies.at[donor].add(-shifted).at[sink].add(shifted)
    labels = jnp.searchsorted(jnp.cumsum(tallies), jnp.arange(rows * top), side="right").astype(jnp.int32)
    table = labels.reshape(top, rows).T
    table = table[jax.random.permutation(jax.random.fold_in(own, 1), rows)]
    rotation = jax.random.randint(jax.random.fold_in(own, 2), (rows, 1), 0, top)
    return jnp.take_along_axis(table, (jnp.arange(top)[None, :] + rotation) % top, axis=1)


def shares(count, total, bound, lean, full):
    weights = [(1 << 20) // math.isqrt(rank ** lean) + 1 for rank in range(1, count + 1)]
    largest = bound if full else min(bound, max(-(-total // count), total * weights[0] // sum(weights)))
    least = 1 if total - largest >= count - 1 else 0
    counts, spare = [largest] + [least] * (count - 1), total - largest - least * (count - 1)
    while spare > 0:
        candidates = [i for i in range(1, count) if counts[i] < largest] or [i for i in range(1, count) if counts[i] < bound]
        pool, left = sum([weights[i] for i in candidates]), spare
        for i in candidates:
            more = min(bound - counts[i], max(1, left * weights[i] // pool), spare)
            counts[i] = counts[i] + more
            spare = spare - more
    return np.array(counts)


def normal_values(key, shape, spread, reach, cuts=(), kind=jnp.bfloat16):
    values = spread * jax.random.normal(key, shape, jnp.float32)
    if cuts:
        values = values * block_levels(key, shape, cuts, -0.22, 0.18)
    return jnp.clip(values, -reach, reach).astype(kind)


def setup_inputs(seed: int = 0) -> dict:
    key_list = jax.random.split(jax.random.key(seed), 22)
    wide_inputs = normal_values(key_list[0], (TOKENS, SETW), 1.0, 6.0, ((0, 64), (1, 2)))
    narrow_inputs = normal_values(key_list[1], (TOKENS, SETW), 1.0, 6.0, ((0, 64), (1, 2)))
    wide_poles = draw_wide_poles(jax.random.fold_in(key_list[21], 71), 0)
    narrow_poles = draw_narrow_poles(jax.random.fold_in(key_list[21], 71), 0)
    step_sizes = draw_step_sizes(jax.random.fold_in(key_list[21], 71), 0)
    forget = draw_forget(jax.random.fold_in(key_list[21], 71), 0)
    wide_in_map = normal_values(key_list[6], (2, 2, GROUPS, CHANNELS, WIDE_STATE), ((2 * CHANNELS) ** -0.5), 2.5, ((2, 2),), jnp.float32)
    narrow_in_map = normal_values(key_list[7], (2, 2, GROUPS, CHANNELS, NARROW_STATE), ((2 * CHANNELS) ** -0.5), 2.5, ((2, 2),), jnp.float32)
    wide_out_map = normal_values(key_list[8], (2, 2, GROUPS, CHANNELS, WIDE_STATE), ((2 * WIDE_STATE) ** -0.5), 1.25, ((2, 2),), jnp.float32)
    narrow_out_map = normal_values(key_list[9], (2, 2, GROUPS, CHANNELS, NARROW_STATE), ((2 * NARROW_STATE) ** -0.5), 2.0, ((2, 2),), jnp.float32)
    skip_weight = normal_values(key_list[10], (2, SETW), 1.0, 6.0, ((1, 2),))
    gate_mix = normal_values(key_list[11], (2, GROUPS, CHANNELS, CHANNELS), CHANNELS ** -0.5, 1.5, ((1, 2),))
    residual = normal_values(key_list[12], (TOKENS, D), 1.0, 6.0, ((0, 128),))
    mixer_gain = jnp.clip(1.0 + 0.18 * jax.random.normal(key_list[13], (2 * SETW,), jnp.float32), 0.1, 1.9)
    out_proj = normal_values(key_list[14], (2 * SETW, D), (2 * SETW) ** -0.5, 0.1875)
    ffn_gain = jnp.clip(1.0 + 0.18 * jax.random.normal(key_list[15], (D,), jnp.float32), 0.1, 1.9)
    routes_keys = jax.random.split(jax.random.fold_in(key_list[16], 1), TOKENS // ROWS)
    routes_turns = jax.random.permutation(jax.random.fold_in(key_list[16], 3), TOKENS // ROWS)
    routes = jax.vmap(lambda own, number: assign_block(jax.random.fold_in(key_list[16], 2), own, number, ROWS, EXPERTS, TOP, CAP, 2))(routes_keys, routes_turns).reshape((TOKENS, TOP))
    route_weights = jnp.clip(jnp.exp(math.log(1.0) - 2.3025851 * jax.random.uniform(key_list[17], (TOKENS, TOP), jnp.float32) ** block_levels(key_list[17], (TOKENS, TOP), ((0, 128),), -0.2, 0.2)), 0.1, 1.0)
    gate_proj = normal_values(key_list[18], (EXPERTS, D, FE), D ** -0.5, 0.125, ((0, 128),))
    up_proj = normal_values(key_list[19], (EXPERTS, D, FE), D ** -0.5, 0.125, ((0, 128),))
    down_proj = normal_values(key_list[20], (EXPERTS, FE, D), FE ** -0.5, 0.15625, ((0, 128),))
    return dict(wide_inputs=wide_inputs, narrow_inputs=narrow_inputs, wide_poles=wide_poles, narrow_poles=narrow_poles, step_sizes=step_sizes, forget=forget, wide_in_map=wide_in_map, narrow_in_map=narrow_in_map, wide_out_map=wide_out_map, narrow_out_map=narrow_out_map, skip_weight=skip_weight, gate_mix=gate_mix, residual=residual, mixer_gain=mixer_gain, out_proj=out_proj, ffn_gain=ffn_gain, routes=routes, route_weights=route_weights, gate_proj=gate_proj, up_proj=up_proj, down_proj=down_proj)


maximum_value = lax.Precision.HIGHEST
epsilon = 1e-06

def pair_step(first, second):
    first_ar, first_ai, first_br, first_bi = first
    second_ar, second_ai, second_br, second_bi = second
    return (second_ar * first_ar - second_ai * first_ai, second_ar * first_ai + second_ai * first_ar, second_ar * first_br - second_ai * first_bi + second_br, second_ar * first_bi + second_ai * first_br + second_bi)

def block_diagonal_in(matrix):
    groups, channels, states = matrix.shape
    identity = jnp.eye(groups, dtype=jnp.float32)
    return jnp.einsum('gcs,gh->gchs', matrix, identity).reshape(groups * channels, groups * states)

def block_diagonal_out(matrix):
    groups, channels, states = matrix.shape
    identity = jnp.eye(groups, dtype=jnp.float32)
    return jnp.einsum('gcs,gh->gshc', matrix, identity).reshape(groups * states, groups * channels)

def local_states(input_sequence, poles, step, decay, in_map, backward):
    decay_re = poles[0]
    decay_im = poles[1]
    states = decay_re.shape[1]
    growth = jnp.exp(decay_re)
    numer_re = growth * jnp.cos(decay_im) - 1.0
    numer_im = growth * jnp.sin(decay_im)
    denom = decay_re * decay_re + decay_im * decay_im
    factor_re = (numer_re * decay_re + numer_im * decay_im) / denom * step[:, None]
    factor_im = (numer_im * decay_re - numer_re * decay_im) / denom * step[:, None]
    input_real = factor_re[:, None, :] * in_map[0] - factor_im[:, None, :] * in_map[1]
    input_imaginary = factor_re[:, None, :] * in_map[1] + factor_im[:, None, :] * in_map[0]
    driven_real = jnp.dot(input_sequence, block_diagonal_in(input_real), precision=maximum_value)
    driven_imaginary = jnp.dot(input_sequence, block_diagonal_in(input_imaginary), precision=maximum_value)
    flat_re = decay_re.reshape(-1)[None]
    flat_im = decay_im.reshape(-1)[None]
    magnitude = jnp.exp(flat_re - jnp.repeat(jnp.transpose(decay), states, axis=1))
    return lax.associative_scan(pair_step, (magnitude * jnp.cos(flat_im), magnitude * jnp.sin(flat_im), driven_real, driven_imaginary), reverse=backward, axis=0)

def read_out(hidden_state_real, hidden_state_imaginary, output_matrix):
    return jnp.dot(hidden_state_real, block_diagonal_out(output_matrix[0]), precision=maximum_value) - jnp.dot(hidden_state_imaginary, block_diagonal_out(output_matrix[1]), precision=maximum_value)

def finish_set(input_sequence, total, skip_row, gate_block):
    shaped = total + skip_row.astype(jnp.float32)[None] * input_sequence
    active = jax.nn.gelu(shaped, approximate=True)
    gate_full = block_diagonal_in(gate_block.astype(jnp.float32))
    opened = jax.nn.sigmoid(jnp.dot(active, gate_full, precision=maximum_value))
    return (active * opened).astype(jnp.bfloat16)

def run_set(inputs, poles, steps, decay, in_map, output_matrix, skip_row, gate_block):
    blocks = TOKENS // TOK_DEV
    groups = poles.shape[2]
    states = poles.shape[3]
    input_sequence = inputs.astype(jnp.float32)
    signal_blocks = input_sequence.reshape(blocks, TOK_DEV, groups * CHANNELS)
    total = jnp.zeros((TOKENS, groups * CHANNELS), jnp.float32)
    for direction in range(2):
        decay_blocks = jnp.transpose(decay[direction].reshape(groups, blocks, TOK_DEV), (1, 0, 2))
        backward = direction == 1
        edge = 0 if backward else -1

        def stepper(carry, pieces):
            piece, piece_decay = pieces
            prod_re, prod_im, hidden_state_real, hidden_state_imaginary = local_states(piece, poles[direction], steps[direction], piece_decay, in_map[direction], backward)
            full_re = hidden_state_real + prod_re * carry[0][None] - prod_im * carry[1][None]
            full_im = hidden_state_imaginary + prod_re * carry[1][None] + prod_im * carry[0][None]
            return ((full_re[edge], full_im[edge]), read_out(full_re, full_im, output_matrix[direction]))
        start = (jnp.zeros((groups * states,), jnp.float32), jnp.zeros((groups * states,), jnp.float32))
        _, outputs = lax.scan(stepper, start, (signal_blocks, decay_blocks), reverse=backward)
        total = total + outputs.reshape(TOKENS, groups * CHANNELS)
    return finish_set(input_sequence, total, skip_row, gate_block)

def reference(wide_inputs, narrow_inputs, wide_poles, narrow_poles, step_sizes, forget, wide_in_map, narrow_in_map, wide_out_map, narrow_out_map, skip_weight, gate_mix, residual, mixer_gain, out_proj, ffn_gain, routes, route_weights, gate_proj, up_proj, down_proj):
    wide_mix = run_set(wide_inputs, wide_poles, step_sizes[:, 0], forget[:, 0], wide_in_map, wide_out_map, skip_weight[0], gate_mix[0])
    narrow_mix = run_set(narrow_inputs, narrow_poles, step_sizes[:, 1], forget[:, 1], narrow_in_map, narrow_out_map, skip_weight[1], gate_mix[1])
    joined = jnp.concatenate([wide_mix, narrow_mix], axis=1).astype(jnp.float32)
    scale = lax.rsqrt(lax.optimization_barrier(jnp.mean(joined * joined, axis=1, keepdims=True)) + epsilon)
    mixed = (joined * scale * mixer_gain).astype(jnp.bfloat16)
    projected = jnp.dot(mixed, out_proj, preferred_element_type=jnp.float32)
    hidden1 = (residual.astype(jnp.float32) + projected).astype(jnp.bfloat16)
    hidden_wide = hidden1.astype(jnp.float32)
    normed = (hidden_wide * lax.rsqrt(lax.optimization_barrier(jnp.mean(hidden_wide * hidden_wide, axis=1, keepdims=True)) + epsilon) * ffn_gain).astype(jnp.bfloat16)
    share = route_weights / lax.optimization_barrier(jnp.sum(route_weights, axis=1, keepdims=True))
    blocks = TOKENS // ROWS
    picks = routes.reshape(blocks, ROWS * TOP)
    onehot = (picks[:, :, None] == jnp.arange(EXPERTS, dtype=jnp.int32)[None, None, :]).astype(jnp.int32)
    rank = lax.optimization_barrier(jnp.sum((jnp.cumsum(onehot, axis=1) - onehot) * onehot, axis=2))
    anchor = (jnp.arange(blocks, dtype=jnp.int32) * CAP)[:, None]
    place = (picks * (blocks * CAP) + anchor + rank).reshape(-1).astype(jnp.int32)
    sectioning = jnp.zeros((EXPERTS * blocks * CAP, D), jnp.bfloat16).at[place].set(jnp.repeat(normed, TOP, axis=0))

    def apply_expert(pieces):
        rows_in, gate_w, up_w, down_w = pieces
        gate_val = jnp.dot(rows_in, gate_w, preferred_element_type=jnp.float32)
        up_val = jnp.dot(rows_in, up_w, preferred_element_type=jnp.float32)
        expert_hidden = (jax.nn.silu(gate_val) * up_val).astype(jnp.bfloat16)
        return jnp.dot(expert_hidden, down_w, preferred_element_type=jnp.float32).astype(jnp.bfloat16)
    served = lax.map(apply_expert, (sectioning.reshape(EXPERTS, blocks * CAP, D), gate_proj, up_proj, down_proj))
    taken = jnp.take(served.reshape(-1, D), place, axis=0).reshape(TOKENS, TOP, D).astype(jnp.float32)
    result = hidden1.astype(jnp.float32) + lax.optimization_barrier(jnp.sum(share[:, :, None] * taken, axis=1))
    return result.astype(jnp.bfloat16)
```

```python
import functools

import jax
import jax.numpy as jnp
from jax import lax
from jax.experimental import pallas as pl
from jax.experimental.pallas import tpu as pltpu
from jax.sharding import PartitionSpec as P

epsilon = 1e-06
SIDE = 4
SUB = 8
LANES = 128
EXACT = lax.Precision.HIGHEST
F32 = jnp.float32
BF16 = jnp.bfloat16
MESH = pl.DeviceIdType.MESH


def iota(shape, dim):
    return lax.broadcasted_iota(jnp.int32, shape, dim)


def ones_where(mask, dtype=F32):
    return jnp.where(mask, 1.0, 0.0).astype(dtype)


def dot(a, b, contract=((1,), (0,)), precision=None):
    return lax.dot_general(a, b, (contract, ((), ())), precision=precision, preferred_element_type=F32)


def sine_cosine(angle):
    y = angle * 0.25
    q = y * y
    s = y * (1.0 + q * (-1 / 6 + q * (1 / 120 + q * (-1 / 5040 + q * (1 / 362880)))))
    c = 1.0 + q * (-0.5 + q * (1 / 24 + q * (-1 / 720 + q * (1 / 40320 + q * (-1 / 3628800)))))
    for _ in range(2):
        s, c = 2.0 * s * c, 1.0 - 2.0 * s * s
    return s, c


def square(re, im):
    return re * re - im * im, 2.0 * re * im


def times(a, b):
    return a[0] * b[0] - a[1] * b[1], a[0] * b[1] + a[1] * b[0]


def plus(a, b):
    return a[0] + b[0], a[1] + b[1]


def spread(rows, mask):
    copies = mask.shape[1] // rows.shape[1]
    tiled = jnp.concatenate([rows] * copies, axis=1)
    return jnp.where(mask, tiled, 0.0).astype(BF16)


def steps_of(count, direction):
    return range(count) if direction == 0 else range(count - 1, -1, -1)


def layer_kernel(
    wide_u, narrow_u, wide_poles, narrow_poles, step_sizes, forget, wide_in, narrow_in, wide_out,
    narrow_out, skip, gate_mix, residual, mixer_gain, ffn_gain, routes, route_weights, out_proj,
    gate_proj, up_proj, down_proj,
    out_ref,
    proj_v, gate_v, up_v, down_v, push, scaled, shrink, plain, leave, gates, ends, before, recv_ends,
    msg, states, woven, halves, pair, sec, arrived, rows_v, hidden_v, served, returned,
    weight_sem, scan_send, scan_recv, pair_sem, send_sem, recv_sem, back_send, back_recv, self_sem,
):
    n_sp = lax.axis_size("sp")
    sp = lax.axis_index("sp")
    tp = lax.axis_index("tp")
    mine = sp * 2 + tp
    n_dev = n_sp * 2

    barrier = pltpu.get_barrier_semaphore()

    def greet(k, _):
        other = lax.rem(mine + k, n_dev)
        pl.semaphore_signal(
            barrier, inc=1, device_id={"sp": other // 2, "tp": lax.rem(other, 2)}, device_id_type=MESH
        )
        return 0

    lax.fori_loop(1, n_dev, greet, 0)
    fetches = [
        pltpu.make_async_copy(source, target, weight_sem.at[i])
        for i, (source, target) in enumerate(
            ((out_proj, proj_v), (gate_proj.at[0], gate_v), (up_proj.at[0], up_v), (down_proj.at[0], down_v))
        )
    ]
    for fetch in fetches:
        fetch.start()

    tokens = wide_u.shape[0]
    steps = tokens // SUB
    sets = (
        (wide_u, wide_poles, wide_in, wide_out),
        (narrow_u, narrow_poles, narrow_in, narrow_out),
    )
    groups, channels = wide_in.shape[2], wide_in.shape[3]
    width = groups * channels
    per = LANES // channels
    states_of = [each[2].shape[4] for each in sets]
    bases = [0, groups * states_of[0]]
    total = groups * sum(states_of)
    packs = []
    for s in range(2):
        for q in range(groups // per):
            packs.append((s, q, s * width + q * LANES, bases[s] + q * per * states_of[s], per * states_of[s]))

    row = iota((tokens, tokens), 0)
    col = iota((tokens, tokens), 1)
    weave = ones_where(col == lax.rem(row, SUB) * steps + row // SUB, BF16)
    unweave = ones_where(col == lax.rem(row, steps) * SUB + row // steps, BF16)
    same = (col // steps) == lax.rem(row, SUB)
    reach = (
        ones_where(same & (lax.rem(col, steps) <= row // SUB)),
        ones_where(same & (lax.rem(col, steps) >= row // SUB)),
    )
    for s in range(2):
        plain[:, s * width : (s + 1) * width] = dot(weave, sets[s][0][...])
    to_channel = ones_where(iota((2 * groups, 2 * width), 0) == iota((2 * groups, 2 * width), 1) // channels)
    lane = iota((2 * groups, total), 1)
    owner = jnp.where(
        lane < bases[1], lane // states_of[0], groups + (lane - bases[1]) // states_of[1]
    )
    to_lane = ones_where(iota((2 * groups, total), 0) == owner)
    kept = []
    for d in range(2):
        flat = forget[d].reshape(2 * groups, tokens)
        lost = dot(reach[d], flat, ((1,), (1,)), EXACT)
        wide = dot(lost, to_channel, precision=EXACT)
        shrink[d] = jnp.exp(-wide)
        scaled[d] = (plain[...] * jnp.exp(wide)).astype(BF16)
        last = lost[tokens - SUB :] if d == 0 else lost[:SUB]
        kept.append(jnp.exp(-dot(last, to_lane, precision=EXACT)))

    masks = [
        (iota((LANES, per * st), 0) // channels) == (iota((LANES, per * st), 1) // st) for st in states_of
    ]
    eye = iota((groups, groups), 0) == iota((groups, groups), 1)
    rates = [[], []]
    for s in range(2):
        _, poles, in_map, out_map = sets[s]
        st = states_of[s]
        for d in range(2):
            re, im = poles[d, 0], poles[d, 1]
            growth = jnp.exp(re)
            sine, cosine = sine_cosine(im)
            rate = (growth * cosine, growth * sine)
            numer_re, numer_im = rate[0] - 1.0, rate[1]
            step = jnp.sum(jnp.where(eye, step_sizes[d, s : s + 1, :], 0.0), axis=1, keepdims=True)
            over = step / (re * re + im * im)
            factor_re = (numer_re * re + numer_im * im) * over
            factor_im = (numer_im * re - numer_re * im) * over
            flat_mask = iota((groups, groups * st), 0) == iota((groups, groups * st), 1) // st
            rates[d].append(
                [
                    jnp.sum(
                        jnp.where(flat_mask, jnp.concatenate([part] * groups, axis=1), 0.0),
                        axis=0,
                        keepdims=True,
                    )
                    for part in rate
                ]
            )
            m_re, m_im = in_map[d, 0], in_map[d, 1]
            f_re, f_im = factor_re[:, None, :], factor_im[:, None, :]
            enter = (
                (f_re * m_re - f_im * m_im).reshape(width, st),
                (f_re * m_im + f_im * m_re).reshape(width, st),
            )
            for which, q, chan, column, lanes in packs:
                if which != s:
                    continue
                for part in range(2):
                    push[d, part, :, column : column + lanes] = dot(
                        scaled[d, :, chan : chan + LANES],
                        spread(enter[part][q * LANES : (q + 1) * LANES], masks[s]),
                    )
    rate_all = [
        [jnp.concatenate([rates[d][0][part], rates[d][1][part]], axis=1) for part in range(2)]
        for d in range(2)
    ]

    for _, _, _, column, lanes in packs:
        cols = slice(column, column + lanes)
        for d in range(2):
            r_re, r_im = rate_all[d][0][:, cols], rate_all[d][1][:, cols]
            h_re = h_im = None
            for step in steps_of(steps, d):
                at = slice(step * SUB, (step + 1) * SUB)
                p_re, p_im = push[d, 0, at, cols], push[d, 1, at, cols]
                if h_re is None:
                    h_re, h_im = p_re, p_im
                else:
                    h_re, h_im = r_re * h_re - r_im * h_im + p_re, r_re * h_im + r_im * h_re + p_im
            ends[d, 0, :, cols] = h_re
            ends[d, 1, :, cols] = h_im

    sub = iota((SUB, total), 0)
    message = []
    for d in range(2):
        power = tuple(rate_all[d])
        taken = 1
        while taken < steps:
            power = square(*power)
            taken *= 2
        a = (power[0] * kept[d], power[1] * kept[d])
        b = (ends[d, 0] * kept[d], ends[d, 1] * kept[d])

        def moved(value, by, fill):
            shift = by if d == 0 else SUB - by
            fine = sub >= by if d == 0 else sub < SUB - by
            return jnp.where(fine, pltpu.roll(value, shift, 0), fill)

        by = 1
        while by < SUB:
            pa = (moved(a[0], by, 1.0), moved(a[1], by, 0.0))
            pb = (moved(b[0], by, 0.0), moved(b[1], by, 0.0))
            b = plus(times(a, pb), b)
            a = times(a, pa)
            by *= 2
        before[d, 0] = moved(a[0], 1, 1.0)
        before[d, 1] = moved(a[1], 1, 0.0)
        before[d, 2] = moved(b[0], 1, 0.0)
        before[d, 3] = moved(b[1], 1, 0.0)
        edge = slice(SUB - 1, SUB) if d == 0 else slice(0, 1)
        message.append(((a[0][edge], a[1][edge]), (b[0][edge], b[1][edge])))

    pl.semaphore_wait(barrier, n_dev - 1)
    carry = [None, None]
    scan_copies = []
    for stage in range(3):
        stride = SIDE**stage
        place = lax.rem(sp // stride, SIDE)
        rows = [part for d in range(2) for pairs in message[d] for part in pairs]
        block = jnp.concatenate(rows, axis=0)
        msg[stage] = block.astype(BF16)
        copies = []
        for k in range(1, SIDE):
            there = lax.rem(place + k, SIDE)
            copy = pltpu.make_async_remote_copy(
                src_ref=msg.at[stage],
                dst_ref=recv_ends.at[stage, place],
                send_sem=scan_send.at[stage * SIDE + k],
                recv_sem=scan_recv.at[stage * SIDE + k],
                device_id={"sp": sp + (there - place) * stride, "tp": tp},
                device_id_type=MESH,
            )
            copy.start()
            copies.append(copy)
        recv_ends[stage, place] = block.astype(BF16)
        if stage == 0:
            for s in range(2):
                for d in range(2):
                    for part in range(2):
                        rows = sets[s][3][d, part].reshape(width, states_of[s])
                        if part:
                            rows = -rows
                        for which, q, _, column, lanes in packs:
                            if which == s:
                                begin = 2 * column + part * lanes
                                leave[d, :, begin : begin + lanes] = spread(
                                    rows[q * LANES : (q + 1) * LANES], masks[s]
                                )
                gate_rows = gate_mix[s].astype(F32).reshape(width, channels)
                gate_mask = (iota((LANES, LANES), 0) // channels) == (iota((LANES, LANES), 1) // channels)
                for q in range(groups // per):
                    gates[s * (groups // per) + q] = spread(
                        gate_rows[q * LANES : (q + 1) * LANES], gate_mask
                    )
        for copy in copies:
            copy.wait_recv()
        scan_copies += copies
        fetched = [recv_ends[stage, j].astype(F32) for j in range(SIDE)]
        for d in range(2):
            one = jnp.ones((1, total), F32)
            zero = jnp.zeros((1, total), F32)
            pre_a, pre_b = (one, zero), (zero, zero)
            tot_a, tot_b = None, None
            for j in steps_of(SIDE, d):
                use = (j < place) if d == 0 else (j > place)
                parts = [fetched[j][4 * d + r : 4 * d + r + 1] for r in range(4)]
                a, b = tuple(parts[:2]), tuple(parts[2:])
                if tot_a is None:
                    tot_a, tot_b = a, b
                else:
                    tot_a, tot_b = times(a, tot_a), plus(times(a, tot_b), b)
                pre_a = tuple(jnp.where(use, new, old) for new, old in zip(tot_a, pre_a))
                pre_b = tuple(jnp.where(use, new, old) for new, old in zip(tot_b, pre_b))
            message[d] = (tot_a, tot_b)
            if carry[d] is None:
                carry[d] = (pre_a, pre_b)
            else:
                carry[d] = (times(carry[d][0], pre_a), plus(times(carry[d][0], pre_b), carry[d][1]))

    for d in range(2):
        c_re, c_im = carry[d][1]
        a_re, a_im = before[d, 0], before[d, 1]
        ends[d, 0] = a_re * c_re - a_im * c_im + before[d, 2]
        ends[d, 1] = a_re * c_im + a_im * c_re + before[d, 3]

    for index, (s, q, chan, column, lanes) in enumerate(packs):
        cols = slice(column, column + lanes)
        chans = slice(chan, chan + LANES)
        read = skip[s : s + 1, q * LANES : (q + 1) * LANES].astype(F32) * plain[:, chans]
        for d in range(2):
            r_re, r_im = rate_all[d][0][:, cols], rate_all[d][1][:, cols]
            h_re, h_im = ends[d, 0, :, cols], ends[d, 1, :, cols]
            held = None
            for step in steps_of(steps, d):
                at = slice(step * SUB, (step + 1) * SUB)
                p_re, p_im = push[d, 0, at, cols], push[d, 1, at, cols]
                h_re, h_im = r_re * h_re - r_im * h_im + p_re, r_re * h_im + r_im * h_re + p_im
                if held is None:
                    held = (h_re, h_im)
                else:
                    low = min(step, step + 1 if d else step - 1) * SUB
                    for part, new in enumerate((h_re, h_im)):
                        both = [held[part], new] if d == 0 else [new, held[part]]
                        states[d, low : low + 2 * SUB, part * lanes : (part + 1) * lanes] = (
                            jnp.concatenate(both, axis=0).astype(BF16)
                        )
                    held = None
            term = dot(
                states[d, :, : 2 * lanes], leave[d, :, 2 * column : 2 * column + 2 * lanes], ((1,), (1,))
            )
            read = read + shrink[d, :, chans] * term
        active = jax.nn.gelu(read, approximate=True)
        opened = jax.nn.sigmoid(dot(active.astype(BF16), gates[index]))
        woven[:, chans] = (active * opened).astype(BF16)

    half = tokens // 2
    halves[...] = dot(unweave, woven[...]).astype(BF16).reshape(halves.shape)
    swap = pltpu.make_async_remote_copy(
        src_ref=halves.at[1 - tp],
        dst_ref=pair.at[tp],
        send_sem=pair_sem.at[0],
        recv_sem=pair_sem.at[1],
        device_id={"sp": sp, "tp": 1 - tp},
        device_id_type=MESH,
    )
    swap.start()
    pair[tp] = halves[tp]
    picks = iota((2 * n_dev, half), 0) // 2
    slot = lax.rem(iota((2 * n_dev, half), 0), 2).astype(F32)
    named = [routes[k : k + 1, :] == picks for k in range(2)]
    any_named = ones_where(named[0] | named[1])
    upper = ones_where(iota((half, half), 0) < iota((half, half), 1), BF16)
    earlier = dot(any_named.astype(BF16), upper)
    chosen = earlier == slot
    spots = jnp.where(chosen, any_named, 0.0).astype(BF16)
    share_sum = route_weights[0:1, :] + route_weights[1:2, :]
    weight = sum(
        jnp.where(named[k] & chosen, route_weights[k : k + 1, :] / share_sum, 0.0) for k in range(2)
    )
    high = weight.astype(BF16)
    low = (weight - high.astype(F32)).astype(BF16)
    fetches[0].wait()
    swap.wait_recv()
    joined = jnp.concatenate(
        [pair[k, :, :width] for k in range(2)] + [pair[k, :, width:] for k in range(2)], axis=1
    ).astype(F32)
    scale = lax.rsqrt(jnp.mean(joined * joined, axis=1, keepdims=True) + epsilon)
    mixed = (joined * scale * mixer_gain[...]).astype(BF16)
    hidden1 = (residual[...].astype(F32) + dot(mixed, proj_v[...])).astype(BF16)
    hidden_wide = hidden1.astype(F32)
    normed = (
        hidden_wide
        * lax.rsqrt(jnp.mean(hidden_wide * hidden_wide, axis=1, keepdims=True) + epsilon)
        * ffn_gain[...]
    ).astype(BF16)
    sec[...] = dot(spots, normed).astype(BF16).reshape(sec.shape)

    def partner(k, flip):
        dz, dy, dx = k // (SIDE * SIDE), lax.rem(k // SIDE, SIDE), lax.rem(k, SIDE)
        z, y, x = sp // (SIDE * SIDE), lax.rem(sp // SIDE, SIDE), lax.rem(sp, SIDE)
        other = (
            lax.rem(z + dz, SIDE) * SIDE * SIDE + lax.rem(y + dy, SIDE) * SIDE + lax.rem(x + dx, SIDE)
        )
        return other, (tp if flip == 0 else 1 - tp)

    own = pltpu.make_async_copy(sec.at[mine], arrived.at[0, sp], self_sem.at[0])
    own.start()
    for flip in range(2):

        def send(k, _):
            other, side = partner(k, flip)
            pltpu.make_async_remote_copy(
                src_ref=sec.at[other * 2 + side],
                dst_ref=arrived.at[flip, sp],
                send_sem=send_sem.at[flip],
                recv_sem=recv_sem.at[flip],
                device_id={"sp": other, "tp": side},
                device_id_type=MESH,
            ).start()
            return 0

        lax.fori_loop(1 - flip, n_sp, send, 0)

    own.wait()
    for fetch in fetches[1:]:
        fetch.wait()
    experts_width = hidden_v.shape[1]
    tile = 256

    def wait_bytes(ref, count, sem):
        pltpu.make_async_copy(ref.at[pl.ds(0, count)], ref.at[pl.ds(0, count)], sem).wait()

    def halfway(begin, size):
        cols = pl.ds(begin, size)
        gate_val = dot(rows_v[...], gate_v[:, cols])
        up_val = dot(rows_v[...], up_v[:, cols])
        hidden_v[:, cols] = (jax.nn.silu(gate_val) * up_val).astype(BF16)

    for flip in range(2):
        wait_bytes(arrived.at[flip], n_sp - 1 + flip, recv_sem.at[flip])
        rows_v[...] = arrived[flip].reshape(rows_v.shape)

        def first(n, _):
            halfway(pl.multiple_of(n * tile, tile), tile)
            return 0

        whole = experts_width // tile
        lax.fori_loop(0, whole, first, 0)
        if experts_width % tile:
            halfway(whole * tile, experts_width % tile)

        def second(n, _):
            cols = pl.ds(pl.multiple_of(n * tile, tile), tile)
            value = dot(hidden_v[...], down_v[:, cols]).astype(BF16)
            served[flip, :, :, cols] = value.reshape(n_sp, 2, tile)
            return 0

        lax.fori_loop(0, served.shape[3] // tile, second, 0)

        def give(k, _):
            other, side = partner(k, flip)
            pltpu.make_async_remote_copy(
                src_ref=served.at[flip, other],
                dst_ref=returned.at[mine],
                send_sem=back_send.at[flip],
                recv_sem=back_recv,
                device_id={"sp": other, "tp": side},
                device_id_type=MESH,
            ).start()
            return 0

        lax.fori_loop(1 - flip, n_sp, give, 0)
        if flip == 0:
            own_back = pltpu.make_async_copy(served.at[0, sp], returned.at[mine], self_sem.at[1])
            own_back.start()

    own_back.wait()
    wait_bytes(returned, n_dev - 1, back_recv)
    back = returned[...].reshape(2 * n_dev, -1)
    summed = dot(high, back, ((0,), (0,))) + dot(low, back, ((0,), (0,)))
    out_ref[...] = (hidden_wide + summed).astype(BF16)

    for copy in scan_copies:
        copy.wait_send()
    swap.wait_send()
    for flip in range(2):
        wait_bytes(sec, n_sp - 1 + flip, send_sem.at[flip])
        wait_bytes(served.at[flip], n_sp - 1 + flip, back_send.at[flip])


def local(
    wide_inputs, narrow_inputs, wide_poles, narrow_poles, step_sizes, forget, wide_in_map,
    narrow_in_map, wide_out_map, narrow_out_map, skip_weight, gate_mix, residual, mixer_gain,
    out_proj, ffn_gain, routes, route_weights, gate_proj, up_proj, down_proj,
):
    n_sp = lax.axis_size("sp")
    n_dev = 2 * n_sp
    tokens, width = wide_inputs.shape
    groups = wide_in_map.shape[2]
    total = groups * (wide_in_map.shape[4] + narrow_in_map.shape[4])
    widest = LANES // wide_in_map.shape[3] * wide_in_map.shape[4]
    rows, model = residual.shape
    fe = gate_proj.shape[2]
    vmem = pl.BlockSpec(memory_space=pltpu.VMEM)
    hbm = pl.BlockSpec(memory_space=pl.ANY)
    dma = pltpu.SemaphoreType.DMA
    return pl.pallas_call(
        layer_kernel,
        out_shape=jax.ShapeDtypeStruct((rows, model), BF16),
        in_specs=[vmem] * 17 + [hbm] * 4,
        out_specs=vmem,
        scratch_shapes=[
            pltpu.VMEM(out_proj.shape, BF16),
            pltpu.VMEM((model, fe), BF16),
            pltpu.VMEM((model, fe), BF16),
            pltpu.VMEM((fe, model), BF16),
            pltpu.VMEM((2, 2, tokens, total), F32),
            pltpu.VMEM((2, tokens, 2 * width), BF16),
            pltpu.VMEM((2, tokens, 2 * width), F32),
            pltpu.VMEM((tokens, 2 * width), F32),
            pltpu.VMEM((2, LANES, 2 * total), BF16),
            pltpu.VMEM((2 * width // LANES, LANES, LANES), BF16),
            pltpu.VMEM((2, 2, SUB, total), F32),
            pltpu.VMEM((2, 4, SUB, total), F32),
            pltpu.VMEM((3, SIDE, SUB, total), BF16),
            pltpu.VMEM((3, SUB, total), BF16),
            pltpu.VMEM((2, tokens, 2 * widest), BF16),
            pltpu.VMEM((tokens, 2 * width), BF16),
            pltpu.VMEM((2, tokens // 2, 2 * width), BF16),
            pltpu.VMEM((2, tokens // 2, 2 * width), BF16),
            pltpu.VMEM((n_dev, 2, model), BF16),
            pltpu.VMEM((2, n_sp, 2, model), BF16),
            pltpu.VMEM((2 * n_sp, model), BF16),
            pltpu.VMEM((2 * n_sp, fe), BF16),
            pltpu.VMEM((2, n_sp, 2, model), BF16),
            pltpu.VMEM((n_dev, 2, model), BF16),
            dma((4,)), dma((3 * SIDE,)), dma((3 * SIDE,)), dma((2,)), dma((2,)), dma((2,)), dma((2,)),
            dma, dma((2,)),
        ],
        compiler_params=pltpu.CompilerParams(
            collective_id=0, has_side_effects=True, vmem_limit_bytes=60 * 1024 * 1024
        ),
        name="layer",
    )(
        wide_inputs, narrow_inputs, wide_poles, narrow_poles, step_sizes, forget, wide_in_map,
        narrow_in_map, wide_out_map, narrow_out_map, skip_weight, gate_mix, residual,
        mixer_gain.reshape(1, -1), ffn_gain.reshape(1, -1), routes.T, route_weights.T, out_proj,
        gate_proj, up_proj, down_proj,
    )


def solution(mesh):
    return jax.shard_map(
        local,
        mesh=mesh,
        in_specs=(
            P("sp", "tp"),
            P("sp", "tp"),
            P(None, None, "tp", None),
            P(None, None, "tp", None),
            P(None, None, "tp"),
            P(None, None, "tp", "sp"),
            P(None, None, "tp", None, None),
            P(None, None, "tp", None, None),
            P(None, None, "tp", None, None),
            P(None, None, "tp", None, None),
            P(None, "tp"),
            P(None, "tp", None, None),
            P(("sp", "tp"), None),
            P(),
            P(),
            P(),
            P(("sp", "tp"), None),
            P(("sp", "tp"), None),
            P(("sp", "tp"), None, None),
            P(("sp", "tp"), None, None),
            P(("sp", "tp"), None, None),
        ),
        out_specs=P(("sp", "tp"), None),
        check_vma=False,
    )
```

```python
import functools

import jax
import jax.numpy as jnp
from jax import lax
from jax.experimental import pallas as pl
from jax.experimental.pallas import tpu as pltpu
from jax.sharding import PartitionSpec as P

epsilon = 1e-06
SIDE = 4
SUB = 8
SMALL = 17
LANES = 128
EXACT = lax.Precision.HIGHEST
F32 = jnp.float32
BF16 = jnp.bfloat16
MESH = pl.DeviceIdType.MESH


def iota(shape, dim):
    return lax.broadcasted_iota(jnp.int32, shape, dim)


def ones_where(mask, dtype=F32):
    return jnp.where(mask, 1.0, 0.0).astype(dtype)


def dot(a, b, contract=((1,), (0,)), precision=None):
    return lax.dot_general(a, b, (contract, ((), ())), precision=precision, preferred_element_type=F32)


def sine_cosine(angle):
    y = angle * 0.25
    q = y * y
    s = y * (1.0 + q * (-1 / 6 + q * (1 / 120 + q * (-1 / 5040 + q * (1 / 362880)))))
    c = 1.0 + q * (-0.5 + q * (1 / 24 + q * (-1 / 720 + q * (1 / 40320 + q * (-1 / 3628800)))))
    for _ in range(2):
        s, c = 2.0 * s * c, 1.0 - 2.0 * s * s
    return s, c


def square(re, im):
    return re * re - im * im, 2.0 * re * im


def times(a, b):
    return a[0] * b[0] - a[1] * b[1], a[0] * b[1] + a[1] * b[0]


def plus(a, b):
    return a[0] + b[0], a[1] + b[1]


def spread(rows, mask):
    copies = mask.shape[1] // rows.shape[1]
    tiled = jnp.concatenate([rows] * copies, axis=1)
    return jnp.where(mask, tiled, 0.0).astype(BF16)


def steps_of(count, direction):
    return range(count) if direction == 0 else range(count - 1, -1, -1)


def layer_kernel(*refs):
    sources, refs = refs[:SMALL], refs[SMALL:]
    (out_proj, gate_proj, up_proj, down_proj, out_ref), refs = refs[:5], refs[5:]
    staged, refs = refs[:SMALL], refs[SMALL:]
    layer_body(sources, staged, out_proj, gate_proj, up_proj, down_proj, out_ref, *refs)


def layer_body(
    sources, staged, out_proj, gate_proj, up_proj, down_proj, out_ref,
    proj_v, gate_v, up_v, down_v, push, scaled, shrink, plain, leave, gates, ends, before, recv_ends,
    msg, states, woven, halves, pair, sec, arrived, rows_v, hidden_v, served, returned,
    weight_sem, scan_send, scan_recv, pair_sem, send_sem, recv_sem, back_send, back_recv, self_sem, small_sem,
):
    (
        wide_u, narrow_u, forget, wide_poles, narrow_poles, step_sizes, wide_in, narrow_in, wide_out,
        narrow_out, gate_mix, skip, routes, route_weights, mixer_gain, ffn_gain, residual,
    ) = staged
    smalls = [
        pltpu.make_async_copy(source, target, small_sem.at[i])
        for i, (source, target) in enumerate(zip(sources, staged))
    ]
    for small in smalls:
        small.start()
    n_sp = lax.axis_size("sp")
    sp = lax.axis_index("sp")
    tp = lax.axis_index("tp")
    mine = sp * 2 + tp
    n_dev = n_sp * 2

    barrier = pltpu.get_barrier_semaphore()

    for stage in range(3):
        stride = SIDE**stage
        place = lax.rem(sp // stride, SIDE)
        for k in range(1, SIDE):
            there = lax.rem(place + k, SIDE)
            pl.semaphore_signal(
                barrier,
                inc=1,
                device_id={"sp": sp + (there - place) * stride, "tp": tp},
                device_id_type=MESH,
            )
    pl.semaphore_signal(barrier, inc=1, device_id={"sp": sp, "tp": 1 - tp}, device_id_type=MESH)
    fetches = [
        pltpu.make_async_copy(source, target, weight_sem.at[i])
        for i, (source, target) in enumerate(
            ((out_proj, proj_v), (gate_proj.at[0], gate_v), (up_proj.at[0], up_v), (down_proj.at[0], down_v))
        )
    ]
    for fetch in fetches:
        fetch.start()

    for small in smalls[:8]:
        small.wait()
    tokens = wide_u.shape[0]
    steps = tokens // SUB
    sets = (
        (wide_u, wide_poles, wide_in, wide_out),
        (narrow_u, narrow_poles, narrow_in, narrow_out),
    )
    groups, channels = wide_in.shape[2], wide_in.shape[3]
    width = groups * channels
    per = LANES // channels
    states_of = [each[2].shape[4] for each in sets]
    bases = [0, groups * states_of[0]]
    total = groups * sum(states_of)
    packs = []
    for s in range(2):
        for q in range(groups // per):
            packs.append((s, q, s * width + q * LANES, bases[s] + q * per * states_of[s], per * states_of[s]))

    row = iota((tokens, tokens), 0)
    col = iota((tokens, tokens), 1)
    weave = ones_where(col == lax.rem(row, SUB) * steps + row // SUB, BF16)
    unweave = ones_where(col == lax.rem(row, steps) * SUB + row // steps, BF16)
    same = (col // steps) == lax.rem(row, SUB)
    reach = (
        ones_where(same & (lax.rem(col, steps) <= row // SUB)),
        ones_where(same & (lax.rem(col, steps) >= row // SUB)),
    )
    for s in range(2):
        plain[:, s * width : (s + 1) * width] = dot(weave, sets[s][0][...])
    to_channel = ones_where(iota((2 * groups, 2 * width), 0) == iota((2 * groups, 2 * width), 1) // channels)
    lane = iota((2 * groups, total), 1)
    owner = jnp.where(
        lane < bases[1], lane // states_of[0], groups + (lane - bases[1]) // states_of[1]
    )
    to_lane = ones_where(iota((2 * groups, total), 0) == owner)
    kept = []
    for d in range(2):
        flat = forget[d].reshape(2 * groups, tokens)
        lost = dot(reach[d], flat, ((1,), (1,)), EXACT)
        wide = dot(lost, to_channel, precision=EXACT)
        shrink[d] = jnp.exp(-wide)
        scaled[d] = (plain[...] * jnp.exp(wide)).astype(BF16)
        last = lost[tokens - SUB :] if d == 0 else lost[:SUB]
        kept.append(jnp.exp(-dot(last, to_lane, precision=EXACT)))

    masks = [
        (iota((LANES, per * st), 0) // channels) == (iota((LANES, per * st), 1) // st) for st in states_of
    ]
    eye = iota((groups, groups), 0) == iota((groups, groups), 1)
    rates = [[], []]
    for s in range(2):
        _, poles, in_map, out_map = sets[s]
        st = states_of[s]
        for d in range(2):
            re, im = poles[d, 0], poles[d, 1]
            growth = jnp.exp(re)
            sine, cosine = sine_cosine(im)
            rate = (growth * cosine, growth * sine)
            numer_re, numer_im = rate[0] - 1.0, rate[1]
            step = jnp.sum(jnp.where(eye, step_sizes[d, s : s + 1, :], 0.0), axis=1, keepdims=True)
            over = step / (re * re + im * im)
            factor_re = (numer_re * re + numer_im * im) * over
            factor_im = (numer_im * re - numer_re * im) * over
            flat_mask = iota((groups, groups * st), 0) == iota((groups, groups * st), 1) // st
            rates[d].append(
                [
                    jnp.sum(
                        jnp.where(flat_mask, jnp.concatenate([part] * groups, axis=1), 0.0),
                        axis=0,
                        keepdims=True,
                    )
                    for part in rate
                ]
            )
            m_re, m_im = in_map[d, 0], in_map[d, 1]
            f_re, f_im = factor_re[:, None, :], factor_im[:, None, :]
            enter = (
                (f_re * m_re - f_im * m_im).reshape(width, st),
                (f_re * m_im + f_im * m_re).reshape(width, st),
            )
            for which, q, chan, column, lanes in packs:
                if which != s:
                    continue
                for part in range(2):
                    push[d, part, :, column : column + lanes] = dot(
                        scaled[d, :, chan : chan + LANES],
                        spread(enter[part][q * LANES : (q + 1) * LANES], masks[s]),
                    )
    rate_all = [
        [jnp.concatenate([rates[d][0][part], rates[d][1][part]], axis=1) for part in range(2)]
        for d in range(2)
    ]

    for _, _, _, column, lanes in packs:
        cols = slice(column, column + lanes)
        for d in range(2):
            r_re, r_im = rate_all[d][0][:, cols], rate_all[d][1][:, cols]
            h_re = h_im = None
            for step in steps_of(steps, d):
                at = slice(step * SUB, (step + 1) * SUB)
                p_re, p_im = push[d, 0, at, cols], push[d, 1, at, cols]
                if h_re is None:
                    h_re, h_im = p_re, p_im
                else:
                    h_re, h_im = r_re * h_re - r_im * h_im + p_re, r_re * h_im + r_im * h_re + p_im
            ends[d, 0, :, cols] = h_re
            ends[d, 1, :, cols] = h_im

    sub = iota((SUB, total), 0)
    message = []
    for d in range(2):
        power = tuple(rate_all[d])
        taken = 1
        while taken < steps:
            power = square(*power)
            taken *= 2
        a = (power[0] * kept[d], power[1] * kept[d])
        b = (ends[d, 0] * kept[d], ends[d, 1] * kept[d])

        def moved(value, by, fill):
            shift = by if d == 0 else SUB - by
            fine = sub >= by if d == 0 else sub < SUB - by
            return jnp.where(fine, pltpu.roll(value, shift, 0), fill)

        by = 1
        while by < SUB:
            pa = (moved(a[0], by, 1.0), moved(a[1], by, 0.0))
            pb = (moved(b[0], by, 0.0), moved(b[1], by, 0.0))
            b = plus(times(a, pb), b)
            a = times(a, pa)
            by *= 2
        before[d, 0] = moved(a[0], 1, 1.0)
        before[d, 1] = moved(a[1], 1, 0.0)
        before[d, 2] = moved(b[0], 1, 0.0)
        before[d, 3] = moved(b[1], 1, 0.0)
        edge = slice(SUB - 1, SUB) if d == 0 else slice(0, 1)
        message.append(((a[0][edge], a[1][edge]), (b[0][edge], b[1][edge])))

    pl.semaphore_wait(barrier, 3 * (SIDE - 1) + 1)
    carry = [None, None]
    scan_copies = []
    for stage in range(3):
        stride = SIDE**stage
        place = lax.rem(sp // stride, SIDE)
        rows = [part for d in range(2) for pairs in message[d] for part in pairs]
        block = jnp.concatenate(rows, axis=0)
        msg[stage] = block.astype(BF16)
        copies = []
        for k in range(1, SIDE):
            there = lax.rem(place + k, SIDE)
            copy = pltpu.make_async_remote_copy(
                src_ref=msg.at[stage],
                dst_ref=recv_ends.at[stage, place],
                send_sem=scan_send.at[stage * SIDE + k],
                recv_sem=scan_recv.at[stage * SIDE + k],
                device_id={"sp": sp + (there - place) * stride, "tp": tp},
                device_id_type=MESH,
            )
            copy.start()
            copies.append(copy)
        recv_ends[stage, place] = block.astype(BF16)
        if stage == 0:
            for small in smalls[8:]:
                small.wait()
            for s in range(2):
                for d in range(2):
                    for part in range(2):
                        rows = sets[s][3][d, part].reshape(width, states_of[s])
                        if part:
                            rows = -rows
                        for which, q, _, column, lanes in packs:
                            if which == s:
                                begin = 2 * column + part * lanes
                                leave[d, :, begin : begin + lanes] = spread(
                                    rows[q * LANES : (q + 1) * LANES], masks[s]
                                )
                gate_rows = gate_mix[s].astype(F32).reshape(width, channels)
                gate_mask = (iota((LANES, LANES), 0) // channels) == (iota((LANES, LANES), 1) // channels)
                for q in range(groups // per):
                    gates[s * (groups // per) + q] = spread(
                        gate_rows[q * LANES : (q + 1) * LANES], gate_mask
                    )
        for copy in copies:
            copy.wait_recv()
        scan_copies += copies
        fetched = [recv_ends[stage, j].astype(F32) for j in range(SIDE)]
        for d in range(2):
            one = jnp.ones((1, total), F32)
            zero = jnp.zeros((1, total), F32)
            pre_a, pre_b = (one, zero), (zero, zero)
            tot_a, tot_b = None, None
            for j in steps_of(SIDE, d):
                use = (j < place) if d == 0 else (j > place)
                parts = [fetched[j][4 * d + r : 4 * d + r + 1] for r in range(4)]
                a, b = tuple(parts[:2]), tuple(parts[2:])
                if tot_a is None:
                    tot_a, tot_b = a, b
                else:
                    tot_a, tot_b = times(a, tot_a), plus(times(a, tot_b), b)
                pre_a = tuple(jnp.where(use, new, old) for new, old in zip(tot_a, pre_a))
                pre_b = tuple(jnp.where(use, new, old) for new, old in zip(tot_b, pre_b))
            message[d] = (tot_a, tot_b)
            if carry[d] is None:
                carry[d] = (pre_a, pre_b)
            else:
                carry[d] = (times(carry[d][0], pre_a), plus(times(carry[d][0], pre_b), carry[d][1]))

    for d in range(2):
        c_re, c_im = carry[d][1]
        a_re, a_im = before[d, 0], before[d, 1]
        ends[d, 0] = a_re * c_re - a_im * c_im + before[d, 2]
        ends[d, 1] = a_re * c_im + a_im * c_re + before[d, 3]

    for index, (s, q, chan, column, lanes) in enumerate(packs):
        cols = slice(column, column + lanes)
        chans = slice(chan, chan + LANES)
        read = skip[s : s + 1, q * LANES : (q + 1) * LANES].astype(F32) * plain[:, chans]
        for d in range(2):
            r_re, r_im = rate_all[d][0][:, cols], rate_all[d][1][:, cols]
            h_re, h_im = ends[d, 0, :, cols], ends[d, 1, :, cols]
            held = None
            for step in steps_of(steps, d):
                at = slice(step * SUB, (step + 1) * SUB)
                p_re, p_im = push[d, 0, at, cols], push[d, 1, at, cols]
                h_re, h_im = r_re * h_re - r_im * h_im + p_re, r_re * h_im + r_im * h_re + p_im
                if held is None:
                    held = (h_re, h_im)
                else:
                    low = min(step, step + 1 if d else step - 1) * SUB
                    for part, new in enumerate((h_re, h_im)):
                        both = [held[part], new] if d == 0 else [new, held[part]]
                        states[d, low : low + 2 * SUB, part * lanes : (part + 1) * lanes] = (
                            jnp.concatenate(both, axis=0).astype(BF16)
                        )
                    held = None
            term = dot(
                states[d, :, : 2 * lanes], leave[d, :, 2 * column : 2 * column + 2 * lanes], ((1,), (1,))
            )
            read = read + shrink[d, :, chans] * term
        active = jax.nn.gelu(read, approximate=True)
        opened = jax.nn.sigmoid(dot(active.astype(BF16), gates[index]))
        woven[:, chans] = (active * opened).astype(BF16)

    half = tokens // 2
    halves[...] = dot(unweave, woven[...]).astype(BF16).reshape(halves.shape)
    swap = pltpu.make_async_remote_copy(
        src_ref=halves.at[1 - tp],
        dst_ref=pair.at[tp],
        send_sem=pair_sem.at[0],
        recv_sem=pair_sem.at[1],
        device_id={"sp": sp, "tp": 1 - tp},
        device_id_type=MESH,
    )
    swap.start()
    pair[tp] = halves[tp]
    picks = iota((2 * n_dev, half), 0) // 2
    slot = lax.rem(iota((2 * n_dev, half), 0), 2).astype(F32)
    named = [routes[k : k + 1, :] == picks for k in range(2)]
    any_named = ones_where(named[0] | named[1])
    upper = ones_where(iota((half, half), 0) < iota((half, half), 1), BF16)
    earlier = dot(any_named.astype(BF16), upper)
    chosen = earlier == slot
    spots = jnp.where(chosen, any_named, 0.0).astype(BF16)
    share_sum = route_weights[0:1, :] + route_weights[1:2, :]
    weight = sum(
        jnp.where(named[k] & chosen, route_weights[k : k + 1, :] / share_sum, 0.0) for k in range(2)
    )
    high = weight.astype(BF16)
    low = (weight - high.astype(F32)).astype(BF16)
    fetches[0].wait()
    swap.wait_recv()
    joined = jnp.concatenate(
        [pair[k, :, :width] for k in range(2)] + [pair[k, :, width:] for k in range(2)], axis=1
    ).astype(F32)
    scale = lax.rsqrt(jnp.mean(joined * joined, axis=1, keepdims=True) + epsilon)
    mixed = (joined * scale * mixer_gain[...]).astype(BF16)
    hidden1 = (residual[...].astype(F32) + dot(mixed, proj_v[...])).astype(BF16)
    hidden_wide = hidden1.astype(F32)
    normed = (
        hidden_wide
        * lax.rsqrt(jnp.mean(hidden_wide * hidden_wide, axis=1, keepdims=True) + epsilon)
        * ffn_gain[...]
    ).astype(BF16)
    sec[...] = dot(spots, normed).astype(BF16).reshape(sec.shape)

    def partner(k, flip):
        dz, dy, dx = k // (SIDE * SIDE), lax.rem(k // SIDE, SIDE), lax.rem(k, SIDE)
        z, y, x = sp // (SIDE * SIDE), lax.rem(sp // SIDE, SIDE), lax.rem(sp, SIDE)
        other = (
            lax.rem(z + dz, SIDE) * SIDE * SIDE + lax.rem(y + dy, SIDE) * SIDE + lax.rem(x + dx, SIDE)
        )
        return other, (tp if flip == 0 else 1 - tp)

    own = pltpu.make_async_copy(sec.at[mine], arrived.at[0, sp], self_sem.at[0])
    own.start()
    for flip in range(2):

        def send(k, _):
            other, side = partner(k, flip)
            pltpu.make_async_remote_copy(
                src_ref=sec.at[other * 2 + side],
                dst_ref=arrived.at[flip, sp],
                send_sem=send_sem.at[flip],
                recv_sem=recv_sem.at[flip],
                device_id={"sp": other, "tp": side},
                device_id_type=MESH,
            ).start()
            return 0

        lax.fori_loop(1 - flip, n_sp, send, 0)

    own.wait()
    for fetch in fetches[1:]:
        fetch.wait()
    def wait_bytes(ref, count, sem):
        pltpu.make_async_copy(ref.at[pl.ds(0, count)], ref.at[pl.ds(0, count)], sem).wait()

    for flip in range(2):
        wait_bytes(arrived.at[flip], n_sp - 1 + flip, recv_sem.at[flip])
        rows_v[...] = arrived[flip].reshape(rows_v.shape)

        gate_val = dot(rows_v[...], gate_v[...])
        up_val = dot(rows_v[...], up_v[...])
        hidden_v[...] = (jax.nn.silu(gate_val) * up_val).astype(BF16)
        served[flip] = dot(hidden_v[...], down_v[...]).astype(BF16).reshape(served.shape[1:])

        def give(k, _):
            other, side = partner(k, flip)
            pltpu.make_async_remote_copy(
                src_ref=served.at[flip, other],
                dst_ref=returned.at[mine],
                send_sem=back_send.at[flip],
                recv_sem=back_recv,
                device_id={"sp": other, "tp": side},
                device_id_type=MESH,
            ).start()
            return 0

        lax.fori_loop(1 - flip, n_sp, give, 0)
        if flip == 0:
            own_back = pltpu.make_async_copy(served.at[0, sp], returned.at[mine], self_sem.at[1])
            own_back.start()

    own_back.wait()
    wait_bytes(returned, n_dev - 1, back_recv)
    back = returned[...].reshape(2 * n_dev, -1)
    summed = dot(high, back, ((0,), (0,))) + dot(low, back, ((0,), (0,)))
    out_ref[...] = (hidden_wide + summed).astype(BF16)

    for copy in scan_copies:
        copy.wait_send()
    swap.wait_send()
    for flip in range(2):
        wait_bytes(sec, n_sp - 1 + flip, send_sem.at[flip])
        wait_bytes(served.at[flip], n_sp - 1 + flip, back_send.at[flip])


def local(
    wide_inputs, narrow_inputs, wide_poles, narrow_poles, step_sizes, forget, wide_in_map,
    narrow_in_map, wide_out_map, narrow_out_map, skip_weight, gate_mix, residual, mixer_gain,
    out_proj, ffn_gain, routes, route_weights, gate_proj, up_proj, down_proj,
):
    n_sp = lax.axis_size("sp")
    n_dev = 2 * n_sp
    tokens, width = wide_inputs.shape
    groups = wide_in_map.shape[2]
    total = groups * (wide_in_map.shape[4] + narrow_in_map.shape[4])
    widest = LANES // wide_in_map.shape[3] * wide_in_map.shape[4]
    rows, model = residual.shape
    fe = gate_proj.shape[2]
    hbm = pl.BlockSpec(memory_space=pltpu.HBM)
    smalls = (
        wide_inputs, narrow_inputs, forget, wide_poles, narrow_poles, step_sizes, wide_in_map,
        narrow_in_map, wide_out_map, narrow_out_map, gate_mix, skip_weight, routes.T,
        route_weights.T, mixer_gain.reshape(1, -1), ffn_gain.reshape(1, -1), residual,
    )
    dma = pltpu.SemaphoreType.DMA
    result = pl.pallas_call(
        layer_kernel,
        out_shape=jax.ShapeDtypeStruct((rows, model), BF16),
        in_specs=[hbm] * (SMALL + 4),
        out_specs=pl.BlockSpec(memory_space=pltpu.VMEM),
        scratch_shapes=[pltpu.VMEM(each.shape, each.dtype) for each in smalls]
        + [
            pltpu.VMEM(out_proj.shape, BF16),
            pltpu.VMEM((model, fe), BF16),
            pltpu.VMEM((model, fe), BF16),
            pltpu.VMEM((fe, model), BF16),
            pltpu.VMEM((2, 2, tokens, total), F32),
            pltpu.VMEM((2, tokens, 2 * width), BF16),
            pltpu.VMEM((2, tokens, 2 * width), F32),
            pltpu.VMEM((tokens, 2 * width), F32),
            pltpu.VMEM((2, LANES, 2 * total), BF16),
            pltpu.VMEM((2 * width // LANES, LANES, LANES), BF16),
            pltpu.VMEM((2, 2, SUB, total), F32),
            pltpu.VMEM((2, 4, SUB, total), F32),
            pltpu.VMEM((3, SIDE, SUB, total), BF16),
            pltpu.VMEM((3, SUB, total), BF16),
            pltpu.VMEM((2, tokens, 2 * widest), BF16),
            pltpu.VMEM((tokens, 2 * width), BF16),
            pltpu.VMEM((2, tokens // 2, 2 * width), BF16),
            pltpu.VMEM((2, tokens // 2, 2 * width), BF16),
            pltpu.VMEM((n_dev, 2, model), BF16),
            pltpu.VMEM((2, n_sp, 2, model), BF16),
            pltpu.VMEM((2 * n_sp, model), BF16),
            pltpu.VMEM((2 * n_sp, fe), BF16),
            pltpu.VMEM((2, n_sp, 2, model), BF16),
            pltpu.VMEM((n_dev, 2, model), BF16),
            dma((4,)), dma((3 * SIDE,)), dma((3 * SIDE,)), dma((2,)), dma((2,)), dma((2,)), dma((2,)),
            dma, dma((2,)), dma((SMALL,)),
        ],
        compiler_params=pltpu.CompilerParams(
            collective_id=0, has_side_effects=True, vmem_limit_bytes=60 * 1024 * 1024
        ),
        name="layer",
    )(*smalls, out_proj, gate_proj, up_proj, down_proj)
    return result


def solution(mesh):
    return jax.shard_map(
        local,
        mesh=mesh,
        in_specs=(
            P("sp", "tp"),
            P("sp", "tp"),
            P(None, None, "tp", None),
            P(None, None, "tp", None),
            P(None, None, "tp"),
            P(None, None, "tp", "sp"),
            P(None, None, "tp", None, None),
            P(None, None, "tp", None, None),
            P(None, None, "tp", None, None),
            P(None, None, "tp", None, None),
            P(None, "tp"),
            P(None, "tp", None, None),
            P(("sp", "tp"), None),
            P(),
            P(),
            P(),
            P(("sp", "tp"), None),
            P(("sp", "tp"), None),
            P(("sp", "tp"), None, None),
            P(("sp", "tp"), None, None),
            P(("sp", "tp"), None, None),
        ),
        out_specs=P(("sp", "tp"), None),
        check_vma=False,
    )
```

```python
import functools

import jax
import jax.numpy as jnp
from jax import lax
from jax.experimental import pallas as pl
from jax.experimental.pallas import tpu as pltpu
from jax.sharding import PartitionSpec as P

epsilon = 1e-06
SIDE = 4
SUB = 8
SMALL = 17
LANES = 128
EXACT = lax.Precision.HIGHEST
F32 = jnp.float32
BF16 = jnp.bfloat16
MESH = pl.DeviceIdType.MESH


def iota(shape, dim):
    return lax.broadcasted_iota(jnp.int32, shape, dim)


def ones_where(mask, dtype=F32):
    return jnp.where(mask, 1.0, 0.0).astype(dtype)


def dot(a, b, contract=((1,), (0,)), precision=None):
    return lax.dot_general(a, b, (contract, ((), ())), precision=precision, preferred_element_type=F32)


def sine_cosine(angle):
    y = angle * 0.25
    q = y * y
    s = y * (1.0 + q * (-1 / 6 + q * (1 / 120 + q * (-1 / 5040 + q * (1 / 362880)))))
    c = 1.0 + q * (-0.5 + q * (1 / 24 + q * (-1 / 720 + q * (1 / 40320 + q * (-1 / 3628800)))))
    for _ in range(2):
        s, c = 2.0 * s * c, 1.0 - 2.0 * s * s
    return s, c


def square(re, im):
    return re * re - im * im, 2.0 * re * im


def times(a, b):
    return a[0] * b[0] - a[1] * b[1], a[0] * b[1] + a[1] * b[0]


def plus(a, b):
    return a[0] + b[0], a[1] + b[1]


def spread(rows, mask):
    copies = mask.shape[1] // rows.shape[1]
    tiled = jnp.concatenate([rows] * copies, axis=1)
    return jnp.where(mask, tiled, 0.0).astype(BF16)


def steps_of(count, direction):
    return range(count) if direction == 0 else range(count - 1, -1, -1)


def layer_kernel(*refs):
    sources, refs = refs[:SMALL], refs[SMALL:]
    (out_proj, gate_proj, up_proj, down_proj, out_ref), refs = refs[:5], refs[5:]
    staged, refs = refs[:SMALL], refs[SMALL:]
    layer_body(sources, staged, out_proj, gate_proj, up_proj, down_proj, out_ref, *refs)


def layer_body(
    sources, staged, out_proj, gate_proj, up_proj, down_proj, out_ref,
    proj_v, gate_v, up_v, down_v, push, scaled, shrink, plain, leave, gates, ends, before, recv_ends,
    msg, states, woven, halves, pair, sec, arrived, rows_v, hidden_v, served, returned,
    weight_sem, scan_send, scan_recv, pair_sem, send_sem, recv_sem, back_send, back_recv, self_sem, small_sem,
):
    (
        wide_u, narrow_u, forget, wide_poles, narrow_poles, step_sizes, wide_in, narrow_in, wide_out,
        narrow_out, gate_mix, skip, routes, route_weights, mixer_gain, ffn_gain, residual,
    ) = staged
    smalls = [
        pltpu.make_async_copy(source, target, small_sem.at[i])
        for i, (source, target) in enumerate(zip(sources, staged))
    ]
    for small in smalls:
        small.start()
    n_sp = lax.axis_size("sp")
    sp = lax.axis_index("sp")
    tp = lax.axis_index("tp")

    barrier = pltpu.get_barrier_semaphore()

    for stage in range(3):
        stride = SIDE**stage
        place = lax.rem(sp // stride, SIDE)
        for k in range(1, SIDE):
            there = lax.rem(place + k, SIDE)
            pl.semaphore_signal(
                barrier,
                inc=1,
                device_id={"sp": sp + (there - place) * stride, "tp": tp},
                device_id_type=MESH,
            )
    pl.semaphore_signal(barrier, inc=1, device_id={"sp": sp, "tp": 1 - tp}, device_id_type=MESH)
    fetches = [
        pltpu.make_async_copy(source, target, weight_sem.at[i])
        for i, (source, target) in enumerate(
            ((out_proj, proj_v), (gate_proj.at[0], gate_v), (up_proj.at[0], up_v), (down_proj.at[0], down_v))
        )
    ]
    for fetch in fetches[:2]:
        fetch.start()

    for small in smalls[:8]:
        small.wait()
    tokens = wide_u.shape[0]
    steps = tokens // SUB
    sets = (
        (wide_u, wide_poles, wide_in, wide_out),
        (narrow_u, narrow_poles, narrow_in, narrow_out),
    )
    groups, channels = wide_in.shape[2], wide_in.shape[3]
    width = groups * channels
    per = LANES // channels
    states_of = [each[2].shape[4] for each in sets]
    bases = [0, groups * states_of[0]]
    total = groups * sum(states_of)
    packs = []
    for s in range(2):
        for q in range(groups // per):
            packs.append((s, q, s * width + q * LANES, bases[s] + q * per * states_of[s], per * states_of[s]))

    row = iota((tokens, tokens), 0)
    col = iota((tokens, tokens), 1)
    weave = ones_where(col == lax.rem(row, SUB) * steps + row // SUB, BF16)
    unweave = ones_where(col == lax.rem(row, steps) * SUB + row // steps, BF16)
    same = (col // steps) == lax.rem(row, SUB)
    reach = (
        ones_where(same & (lax.rem(col, steps) <= row // SUB)),
        ones_where(same & (lax.rem(col, steps) >= row // SUB)),
    )
    for s in range(2):
        plain[:, s * width : (s + 1) * width] = dot(weave, sets[s][0][...])
    to_channel = ones_where(iota((2 * groups, 2 * width), 0) == iota((2 * groups, 2 * width), 1) // channels)
    lane = iota((2 * groups, total), 1)
    owner = jnp.where(
        lane < bases[1], lane // states_of[0], groups + (lane - bases[1]) // states_of[1]
    )
    to_lane = ones_where(iota((2 * groups, total), 0) == owner)
    kept, kept_all = [], []
    for d in range(2):
        flat = forget[d].reshape(2 * groups, tokens)
        lost = dot(reach[d], flat, ((1,), (1,)), EXACT)
        wide = dot(lost, to_channel, precision=EXACT)
        shrink[d] = jnp.exp(-wide)
        scaled[d] = (plain[...] * jnp.exp(wide)).astype(BF16)
        last = lost[tokens - SUB :] if d == 0 else lost[:SUB]
        fall = dot(last, to_lane, precision=EXACT)
        kept.append(jnp.exp(-fall))
        kept_all.append(jnp.exp(-jnp.sum(fall, axis=0, keepdims=True)))

    masks = [
        (iota((LANES, per * st), 0) // channels) == (iota((LANES, per * st), 1) // st) for st in states_of
    ]
    eye = iota((groups, groups), 0) == iota((groups, groups), 1)
    rates = [[], []]
    for s in range(2):
        _, poles, in_map, out_map = sets[s]
        st = states_of[s]
        for d in range(2):
            re, im = poles[d, 0], poles[d, 1]
            growth = jnp.exp(re)
            sine, cosine = sine_cosine(im)
            rate = (growth * cosine, growth * sine)
            numer_re, numer_im = rate[0] - 1.0, rate[1]
            step = jnp.sum(jnp.where(eye, step_sizes[d, s : s + 1, :], 0.0), axis=1, keepdims=True)
            over = step / (re * re + im * im)
            factor_re = (numer_re * re + numer_im * im) * over
            factor_im = (numer_im * re - numer_re * im) * over
            flat_mask = iota((groups, groups * st), 0) == iota((groups, groups * st), 1) // st
            rates[d].append(
                [
                    jnp.sum(
                        jnp.where(flat_mask, jnp.concatenate([part] * groups, axis=1), 0.0),
                        axis=0,
                        keepdims=True,
                    )
                    for part in rate
                ]
            )
            m_re, m_im = in_map[d, 0], in_map[d, 1]
            f_re, f_im = factor_re[:, None, :], factor_im[:, None, :]
            enter = (
                (f_re * m_re - f_im * m_im).reshape(width, st),
                (f_re * m_im + f_im * m_re).reshape(width, st),
            )
            for which, q, chan, column, lanes in packs:
                if which != s:
                    continue
                for part in range(2):
                    push[d, part, :, column : column + lanes] = dot(
                        scaled[d, :, chan : chan + LANES],
                        spread(enter[part][q * LANES : (q + 1) * LANES], masks[s]),
                    )
    rate_all = [
        [jnp.concatenate([rates[d][0][part], rates[d][1][part]], axis=1) for part in range(2)]
        for d in range(2)
    ]

    for _, _, _, column, lanes in packs:
        cols = slice(column, column + lanes)
        for d in range(2):
            r_re, r_im = rate_all[d][0][:, cols], rate_all[d][1][:, cols]
            h_re = h_im = None
            for step in steps_of(steps, d):
                at = slice(step * SUB, (step + 1) * SUB)
                p_re, p_im = push[d, 0, at, cols], push[d, 1, at, cols]
                if h_re is None:
                    h_re, h_im = p_re, p_im
                else:
                    h_re, h_im = r_re * h_re - r_im * h_im + p_re, r_re * h_im + r_im * h_re + p_im
            ends[d, 0, :, cols] = h_re
            ends[d, 1, :, cols] = h_im

    sub = iota((SUB, total), 0)
    message, powers = [], []
    folds = total // LANES

    def fold(value):
        return jnp.concatenate([value[:, i * LANES : (i + 1) * LANES] for i in range(folds)], axis=0)
    for d in range(2):
        power = tuple(rate_all[d])
        taken = 1
        while taken < steps:
            power = square(*power)
            taken *= 2
        a = (power[0] * kept[d], power[1] * kept[d])
        b = (ends[d, 0] * kept[d], ends[d, 1] * kept[d])

        def moved(value, by, fill):
            shift = by if d == 0 else SUB - by
            fine = sub >= by if d == 0 else sub < SUB - by
            return jnp.where(fine, pltpu.roll(value, shift, 0), fill)

        by = 1
        while by < SUB:
            pa = (moved(a[0], by, 1.0), moved(a[1], by, 0.0))
            pb = (moved(b[0], by, 0.0), moved(b[1], by, 0.0))
            b = plus(times(a, pb), b)
            a = times(a, pa)
            by *= 2
        before[d, 0] = moved(a[0], 1, 1.0)
        before[d, 1] = moved(a[1], 1, 0.0)
        before[d, 2] = moved(b[0], 1, 0.0)
        before[d, 3] = moved(b[1], 1, 0.0)
        edge = slice(SUB - 1, SUB) if d == 0 else slice(0, 1)
        message.append((fold(kept_all[d]), (fold(b[0][edge]), fold(b[1][edge]))))
        stride_power = tuple(fold(part) for part in rate_all[d])
        taken = 1
        while taken < tokens:
            stride_power = square(*stride_power)
            taken *= 2
        powers.append(stride_power)

    pl.semaphore_wait(barrier, 3 * (SIDE - 1) + 1)
    carry = [None, None]
    scan_copies = []
    for stage in range(3):
        stride = SIDE**stage
        place = lax.rem(sp // stride, SIDE)
        block = jnp.concatenate([part for k, b in message for part in (k, b[0], b[1])], axis=0)
        msg[stage] = block.astype(BF16)
        copies = []
        for k in range(1, SIDE):
            there = lax.rem(place + k, SIDE)
            copy = pltpu.make_async_remote_copy(
                src_ref=msg.at[stage],
                dst_ref=recv_ends.at[stage, place],
                send_sem=scan_send.at[stage * SIDE + k],
                recv_sem=scan_recv.at[stage * SIDE + k],
                device_id={"sp": sp + (there - place) * stride, "tp": tp},
                device_id_type=MESH,
            )
            copy.start()
            copies.append(copy)
        recv_ends[stage, place] = block.astype(BF16)
        if stage < 2:
            fetches[2 + stage].start()
        if stage == 0:
            for small in smalls[8:]:
                small.wait()
            for s in range(2):
                for d in range(2):
                    for part in range(2):
                        rows = sets[s][3][d, part].reshape(width, states_of[s])
                        if part:
                            rows = -rows
                        for which, q, _, column, lanes in packs:
                            if which == s:
                                begin = 2 * column + part * lanes
                                leave[d, :, begin : begin + lanes] = spread(
                                    rows[q * LANES : (q + 1) * LANES], masks[s]
                                )
                gate_rows = gate_mix[s].astype(F32).reshape(width, channels)
                gate_mask = (iota((LANES, LANES), 0) // channels) == (iota((LANES, LANES), 1) // channels)
                for q in range(groups // per):
                    gates[s * (groups // per) + q] = spread(
                        gate_rows[q * LANES : (q + 1) * LANES], gate_mask
                    )
        for copy in copies:
            copy.wait_recv()
        scan_copies += copies
        fetched = [recv_ends[stage, j].astype(F32) for j in range(SIDE)]
        for d in range(2):
            one = jnp.ones((folds, LANES), F32)
            zero = jnp.zeros((folds, LANES), F32)
            pre_a, pre_b = (one, zero), (zero, zero)
            run_a, tot_k, tot_b = None, None, None
            for j in steps_of(SIDE, d):
                use = (j < place) if d == 0 else (j > place)
                begin = 3 * d * folds
                k, b_re, b_im = (fetched[j][begin + r * folds : begin + (r + 1) * folds] for r in range(3))
                a, b = (powers[d][0] * k, powers[d][1] * k), (b_re, b_im)
                if tot_b is None:
                    run_a, tot_k, tot_b = a, k, b
                else:
                    run_a, tot_k, tot_b = times(a, run_a), k * tot_k, plus(times(a, tot_b), b)
                pre_a = tuple(jnp.where(use, new, old) for new, old in zip(run_a, pre_a))
                pre_b = tuple(jnp.where(use, new, old) for new, old in zip(tot_b, pre_b))
            message[d] = (tot_k, tot_b)
            powers[d] = square(*square(*powers[d]))
            if carry[d] is None:
                carry[d] = (pre_a, pre_b)
            else:
                carry[d] = (times(carry[d][0], pre_a), plus(times(carry[d][0], pre_b), carry[d][1]))

    for d in range(2):
        c_re, c_im = (
            jnp.concatenate([part[i : i + 1] for i in range(folds)], axis=1) for part in carry[d][1]
        )
        a_re, a_im = before[d, 0], before[d, 1]
        ends[d, 0] = a_re * c_re - a_im * c_im + before[d, 2]
        ends[d, 1] = a_re * c_im + a_im * c_re + before[d, 3]

    for index, (s, q, chan, column, lanes) in enumerate(packs):
        cols = slice(column, column + lanes)
        chans = slice(chan, chan + LANES)
        read = skip[s : s + 1, q * LANES : (q + 1) * LANES].astype(F32) * plain[:, chans]
        for d in range(2):
            r_re, r_im = rate_all[d][0][:, cols], rate_all[d][1][:, cols]
            h_re, h_im = ends[d, 0, :, cols], ends[d, 1, :, cols]
            held = None
            for step in steps_of(steps, d):
                at = slice(step * SUB, (step + 1) * SUB)
                p_re, p_im = push[d, 0, at, cols], push[d, 1, at, cols]
                h_re, h_im = r_re * h_re - r_im * h_im + p_re, r_re * h_im + r_im * h_re + p_im
                if held is None:
                    held = (h_re, h_im)
                else:
                    low = min(step, step + 1 if d else step - 1) * SUB
                    for part, new in enumerate((h_re, h_im)):
                        both = [held[part], new] if d == 0 else [new, held[part]]
                        states[d, low : low + 2 * SUB, part * lanes : (part + 1) * lanes] = (
                            jnp.concatenate(both, axis=0).astype(BF16)
                        )
                    held = None
            term = dot(
                states[d, :, : 2 * lanes], leave[d, :, 2 * column : 2 * column + 2 * lanes], ((1,), (1,))
            )
            read = read + shrink[d, :, chans] * term
        active = jax.nn.gelu(read, approximate=True)
        opened = jax.nn.sigmoid(dot(active.astype(BF16), gates[index]))
        woven[:, chans] = (active * opened).astype(BF16)

    half = tokens // 2
    halves[...] = dot(unweave, woven[...]).astype(BF16).reshape(halves.shape)
    swap = pltpu.make_async_remote_copy(
        src_ref=halves.at[1 - tp],
        dst_ref=pair.at[tp],
        send_sem=pair_sem.at[0],
        recv_sem=pair_sem.at[1],
        device_id={"sp": sp, "tp": 1 - tp},
        device_id_type=MESH,
    )
    swap.start()
    pair[tp] = halves[tp]

    def partner(k, flip, sign):
        m = lax.rem(k, n_sp // 2)
        dz, dy = m // (2 * SIDE), lax.rem(m // 2, SIDE)
        dx = 2 * lax.rem(m, 2) + lax.rem(dz + dy + k // (n_sp // 2), 2)
        z, y, x = sp // (SIDE * SIDE), lax.rem(sp // SIDE, SIDE), lax.rem(sp, SIDE)
        z, y, x = (lax.rem(at + sign * by + SIDE, SIDE) for at, by in ((z, dz), (y, dy), (x, dx)))
        return z * SIDE * SIDE + y * SIDE + x, (tp if flip == 0 else 1 - tp)

    upper = ones_where(iota((half, half), 0) < iota((half, half), 1), BF16)
    share_sum = route_weights[0:1, :] + route_weights[1:2, :]
    line = iota((2 * n_sp, half), 0)
    slot = lax.rem(line, 2).astype(F32)
    spots, highs, lows = [], [], []
    for flip in range(2):
        other, side = partner(line // 2, flip, 1)
        picks = other * 2 + side
        named = [routes[k : k + 1, :] == picks for k in range(2)]
        any_named = ones_where(named[0] | named[1])
        chosen = dot(any_named.astype(BF16), upper) == slot
        spots.append(jnp.where(chosen, any_named, 0.0).astype(BF16))
        weight = sum(
            jnp.where(named[k] & chosen, route_weights[k : k + 1, :] / share_sum, 0.0) for k in range(2)
        )
        highs.append(weight.astype(BF16))
        lows.append((weight - highs[flip].astype(F32)).astype(BF16))
    fetches[0].wait()
    swap.wait_recv()
    joined = jnp.concatenate(
        [pair[k, :, :width] for k in range(2)] + [pair[k, :, width:] for k in range(2)], axis=1
    ).astype(F32)
    scale = lax.rsqrt(jnp.mean(joined * joined, axis=1, keepdims=True) + epsilon)
    mixed = (joined * scale * mixer_gain[...]).astype(BF16)
    hidden1 = (residual[...].astype(F32) + dot(mixed, proj_v[...])).astype(BF16)
    hidden_wide = hidden1.astype(F32)
    normed = (
        hidden_wide
        * lax.rsqrt(jnp.mean(hidden_wide * hidden_wide, axis=1, keepdims=True) + epsilon)
        * ffn_gain[...]
    ).astype(BF16)
    for flip in range(2):
        sec[flip] = dot(spots[flip], normed).astype(BF16).reshape(sec.shape[1:])
        if flip == 0:
            own = pltpu.make_async_copy(sec.at[0, 0], arrived.at[0, 0], self_sem.at[0])
            own.start()

        def send(k, _):
            other, side = partner(k, flip, 1)
            pltpu.make_async_remote_copy(
                src_ref=sec.at[flip, k],
                dst_ref=arrived.at[flip, k],
                send_sem=send_sem.at[flip],
                recv_sem=recv_sem.at[flip],
                device_id={"sp": other, "tp": side},
                device_id_type=MESH,
            ).start()
            return 0

        lax.fori_loop(1 - flip, n_sp, send, 0)

    own.wait()
    for fetch in fetches[1:]:
        fetch.wait()
    def wait_bytes(ref, count, sem):
        pltpu.make_async_copy(ref.at[pl.ds(0, count)], ref.at[pl.ds(0, count)], sem).wait()

    for flip in range(2):
        wait_bytes(arrived.at[flip], n_sp - 1 + flip, recv_sem.at[flip])
        rows_v[...] = arrived[flip].reshape(rows_v.shape)

        gate_val = dot(rows_v[...], gate_v[...])
        up_val = dot(rows_v[...], up_v[...])
        hidden_v[...] = (jax.nn.silu(gate_val) * up_val).astype(BF16)
        served[flip] = dot(hidden_v[...], down_v[...]).astype(BF16).reshape(served.shape[1:])

        def give(k, _):
            other, side = partner(k, flip, -1)
            pltpu.make_async_remote_copy(
                src_ref=served.at[flip, k],
                dst_ref=returned.at[flip, k],
                send_sem=back_send.at[flip],
                recv_sem=back_recv.at[flip],
                device_id={"sp": other, "tp": side},
                device_id_type=MESH,
            ).start()
            return 0

        lax.fori_loop(1 - flip, n_sp, give, 0)
        if flip == 0:
            own_back = pltpu.make_async_copy(served.at[0, 0], returned.at[0, 0], self_sem.at[1])
            own_back.start()

    own_back.wait()
    result = hidden_wide
    for flip in range(2):
        wait_bytes(returned.at[flip], n_sp - 1 + flip, back_recv.at[flip])
        back = returned[flip].reshape(2 * n_sp, -1)
        result = result + dot(highs[flip], back, ((0,), (0,))) + dot(lows[flip], back, ((0,), (0,)))
    out_ref[...] = result.astype(BF16)

    for copy in scan_copies:
        copy.wait_send()
    swap.wait_send()
    for flip in range(2):
        wait_bytes(sec.at[flip], n_sp - 1 + flip, send_sem.at[flip])
        wait_bytes(served.at[flip], n_sp - 1 + flip, back_send.at[flip])


def local(
    wide_inputs, narrow_inputs, wide_poles, narrow_poles, step_sizes, forget, wide_in_map,
    narrow_in_map, wide_out_map, narrow_out_map, skip_weight, gate_mix, residual, mixer_gain,
    out_proj, ffn_gain, routes, route_weights, gate_proj, up_proj, down_proj,
):
    n_sp = lax.axis_size("sp")
    tokens, width = wide_inputs.shape
    groups = wide_in_map.shape[2]
    total = groups * (wide_in_map.shape[4] + narrow_in_map.shape[4])
    widest = LANES // wide_in_map.shape[3] * wide_in_map.shape[4]
    rows, model = residual.shape
    fe = gate_proj.shape[2]
    hbm = pl.BlockSpec(memory_space=pltpu.HBM)
    smalls = (
        wide_inputs, narrow_inputs, forget, wide_poles, narrow_poles, step_sizes, wide_in_map,
        narrow_in_map, wide_out_map, narrow_out_map, gate_mix, skip_weight, routes.T,
        route_weights.T, mixer_gain.reshape(1, -1), ffn_gain.reshape(1, -1), residual,
    )
    dma = pltpu.SemaphoreType.DMA
    result = pl.pallas_call(
        layer_kernel,
        out_shape=jax.ShapeDtypeStruct((rows, model), BF16),
        in_specs=[hbm] * (SMALL + 4),
        out_specs=pl.BlockSpec(memory_space=pltpu.VMEM),
        scratch_shapes=[pltpu.VMEM(each.shape, each.dtype) for each in smalls]
        + [
            pltpu.VMEM(out_proj.shape, BF16),
            pltpu.VMEM((model, fe), BF16),
            pltpu.VMEM((model, fe), BF16),
            pltpu.VMEM((fe, model), BF16),
            pltpu.VMEM((2, 2, tokens, total), F32),
            pltpu.VMEM((2, tokens, 2 * width), BF16),
            pltpu.VMEM((2, tokens, 2 * width), F32),
            pltpu.VMEM((tokens, 2 * width), F32),
            pltpu.VMEM((2, LANES, 2 * total), BF16),
            pltpu.VMEM((2 * width // LANES, LANES, LANES), BF16),
            pltpu.VMEM((2, 2, SUB, total), F32),
            pltpu.VMEM((2, 4, SUB, total), F32),
            pltpu.VMEM((3, SIDE, 6 * total // LANES, LANES), BF16),
            pltpu.VMEM((3, 6 * total // LANES, LANES), BF16),
            pltpu.VMEM((2, tokens, 2 * widest), BF16),
            pltpu.VMEM((tokens, 2 * width), BF16),
            pltpu.VMEM((2, tokens // 2, 2 * width), BF16),
            pltpu.VMEM((2, tokens // 2, 2 * width), BF16),
            pltpu.VMEM((2, n_sp, 2, model), BF16),
            pltpu.VMEM((2, n_sp, 2, model), BF16),
            pltpu.VMEM((2 * n_sp, model), BF16),
            pltpu.VMEM((2 * n_sp, fe), BF16),
            pltpu.VMEM((2, n_sp, 2, model), BF16),
            pltpu.VMEM((2, n_sp, 2, model), BF16),
            dma((4,)), dma((3 * SIDE,)), dma((3 * SIDE,)), dma((2,)), dma((2,)), dma((2,)), dma((2,)),
            dma((2,)), dma((2,)), dma((SMALL,)),
        ],
        compiler_params=pltpu.CompilerParams(
            collective_id=0, has_side_effects=True, vmem_limit_bytes=60 * 1024 * 1024
        ),
        name="layer",
    )(*smalls, out_proj, gate_proj, up_proj, down_proj)
    return result


def solution(mesh):
    return jax.shard_map(
        local,
        mesh=mesh,
        in_specs=(
            P("sp", "tp"),
            P("sp", "tp"),
            P(None, None, "tp", None),
            P(None, None, "tp", None),
            P(None, None, "tp"),
            P(None, None, "tp", "sp"),
            P(None, None, "tp", None, None),
            P(None, None, "tp", None, None),
            P(None, None, "tp", None, None),
            P(None, None, "tp", None, None),
            P(None, "tp"),
            P(None, "tp", None, None),
            P(("sp", "tp"), None),
            P(),
            P(),
            P(),
            P(("sp", "tp"), None),
            P(("sp", "tp"), None),
            P(("sp", "tp"), None, None),
            P(("sp", "tp"), None, None),
            P(("sp", "tp"), None, None),
        ),
        out_specs=P(("sp", "tp"), None),
        check_vma=False,
    )
```

```python
import functools

import jax
import jax.numpy as jnp
from jax import lax
from jax.experimental import pallas as pl
from jax.experimental.pallas import tpu as pltpu
from jax.sharding import PartitionSpec as P

epsilon = 1e-06
SIDE = 4
SUB = 8
SMALL = 17
LANES = 128
EXACT = lax.Precision.HIGHEST
F32 = jnp.float32
BF16 = jnp.bfloat16
MESH = pl.DeviceIdType.MESH


def iota(shape, dim):
    return lax.broadcasted_iota(jnp.int32, shape, dim)


def ones_where(mask, dtype=F32):
    return jnp.where(mask, 1.0, 0.0).astype(dtype)


def dot(a, b, contract=((1,), (0,)), precision=None):
    return lax.dot_general(a, b, (contract, ((), ())), precision=precision, preferred_element_type=F32)


def sine_cosine(angle):
    y = angle * 0.25
    q = y * y
    s = y * (1.0 + q * (-1 / 6 + q * (1 / 120 + q * (-1 / 5040 + q * (1 / 362880)))))
    c = 1.0 + q * (-0.5 + q * (1 / 24 + q * (-1 / 720 + q * (1 / 40320 + q * (-1 / 3628800)))))
    for _ in range(2):
        s, c = 2.0 * s * c, 1.0 - 2.0 * s * s
    return s, c


def square(re, im):
    return re * re - im * im, 2.0 * re * im


def times(a, b):
    return a[0] * b[0] - a[1] * b[1], a[0] * b[1] + a[1] * b[0]


def plus(a, b):
    return a[0] + b[0], a[1] + b[1]


def spread(rows, mask):
    copies = mask.shape[1] // rows.shape[1]
    tiled = jnp.concatenate([rows] * copies, axis=1)
    return jnp.where(mask, tiled, 0.0).astype(BF16)


def steps_of(count, direction):
    return range(count) if direction == 0 else range(count - 1, -1, -1)


def layer_kernel(*refs):
    sources, refs = refs[:SMALL], refs[SMALL:]
    (out_proj, gate_proj, up_proj, down_proj, out_ref), refs = refs[:5], refs[5:]
    staged, refs = refs[:SMALL], refs[SMALL:]
    layer_body(sources, staged, out_proj, gate_proj, up_proj, down_proj, out_ref, *refs)


def layer_body(
    sources, staged, out_proj, gate_proj, up_proj, down_proj, out_ref,
    proj_v, gate_v, up_v, down_v, push, scaled, shrink, plain, leave, gates, ends, before, recv_ends,
    msg, states, woven, halves, pair, sec, arrived, rows_v, hidden_v, served, returned,
    weight_sem, scan_send, scan_recv, pair_sem, send_sem, recv_sem, back_send, back_recv, self_sem, small_sem,
):
    (
        wide_u, narrow_u, forget, wide_poles, narrow_poles, step_sizes, wide_in, narrow_in, wide_out,
        narrow_out, gate_mix, skip, routes, route_weights, mixer_gain, ffn_gain, residual,
    ) = staged
    smalls = [
        pltpu.make_async_copy(source, target, small_sem.at[i])
        for i, (source, target) in enumerate(zip(sources, staged))
    ]
    for small in smalls:
        small.start()
    n_sp = lax.axis_size("sp")
    sp = lax.axis_index("sp")
    tp = lax.axis_index("tp")

    barrier = pltpu.get_barrier_semaphore()

    for stage in range(3):
        stride = SIDE**stage
        place = lax.rem(sp // stride, SIDE)
        for k in range(1, SIDE):
            there = lax.rem(place + k, SIDE)
            pl.semaphore_signal(
                barrier,
                inc=1,
                device_id={"sp": sp + (there - place) * stride, "tp": tp},
                device_id_type=MESH,
            )
    pl.semaphore_signal(barrier, inc=1, device_id={"sp": sp, "tp": 1 - tp}, device_id_type=MESH)
    fetches = [
        pltpu.make_async_copy(source, target, weight_sem.at[i])
        for i, (source, target) in enumerate(
            ((out_proj, proj_v), (gate_proj.at[0], gate_v), (up_proj.at[0], up_v), (down_proj.at[0], down_v))
        )
    ]
    for fetch in fetches[:2]:
        fetch.start()

    for small in smalls[:8]:
        small.wait()
    tokens = wide_u.shape[0]
    steps = tokens // SUB
    sets = (
        (wide_u, wide_poles, wide_in, wide_out),
        (narrow_u, narrow_poles, narrow_in, narrow_out),
    )
    groups, channels = wide_in.shape[2], wide_in.shape[3]
    width = groups * channels
    per = LANES // channels
    states_of = [each[2].shape[4] for each in sets]
    bases = [0, groups * states_of[0]]
    total = groups * sum(states_of)
    packs = []
    for s in range(2):
        for q in range(groups // per):
            packs.append((s, q, s * width + q * LANES, bases[s] + q * per * states_of[s], per * states_of[s]))

    row = iota((tokens, tokens), 0)
    col = iota((tokens, tokens), 1)
    weave = ones_where(col == lax.rem(row, SUB) * steps + row // SUB, BF16)
    unweave = ones_where(col == lax.rem(row, steps) * SUB + row // steps, BF16)
    same = (col // steps) == lax.rem(row, SUB)
    reach = (
        ones_where(same & (lax.rem(col, steps) <= row // SUB)),
        ones_where(same & (lax.rem(col, steps) >= row // SUB)),
    )
    for s in range(2):
        plain[:, s * width : (s + 1) * width] = dot(weave, sets[s][0][...])
    to_channel = ones_where(iota((2 * groups, 2 * width), 0) == iota((2 * groups, 2 * width), 1) // channels)
    lane = iota((2 * groups, total), 1)
    owner = jnp.where(
        lane < bases[1], lane // states_of[0], groups + (lane - bases[1]) // states_of[1]
    )
    to_lane = ones_where(iota((2 * groups, total), 0) == owner)
    kept, kept_all = [], []
    for d in range(2):
        flat = forget[d].reshape(2 * groups, tokens)
        lost = dot(reach[d], flat, ((1,), (1,)), EXACT)
        wide = dot(lost, to_channel, precision=EXACT)
        shrink[d] = jnp.exp(-wide)
        scaled[d] = (plain[...] * jnp.exp(wide)).astype(BF16)
        last = lost[tokens - SUB :] if d == 0 else lost[:SUB]
        fall = dot(last, to_lane, precision=EXACT)
        kept.append(jnp.exp(-fall))
        kept_all.append(jnp.exp(-jnp.sum(fall, axis=0, keepdims=True)))

    masks = [
        (iota((LANES, per * st), 0) // channels) == (iota((LANES, per * st), 1) // st) for st in states_of
    ]
    eye = iota((groups, groups), 0) == iota((groups, groups), 1)
    rates = [[], []]
    for s in range(2):
        _, poles, in_map, out_map = sets[s]
        st = states_of[s]
        for d in range(2):
            re, im = poles[d, 0], poles[d, 1]
            growth = jnp.exp(re)
            sine, cosine = sine_cosine(im)
            rate = (growth * cosine, growth * sine)
            numer_re, numer_im = rate[0] - 1.0, rate[1]
            step = jnp.sum(jnp.where(eye, step_sizes[d, s : s + 1, :], 0.0), axis=1, keepdims=True)
            over = step / (re * re + im * im)
            factor_re = (numer_re * re + numer_im * im) * over
            factor_im = (numer_im * re - numer_re * im) * over
            flat_mask = iota((groups, groups * st), 0) == iota((groups, groups * st), 1) // st
            rates[d].append(
                [
                    jnp.sum(
                        jnp.where(flat_mask, jnp.concatenate([part] * groups, axis=1), 0.0),
                        axis=0,
                        keepdims=True,
                    )
                    for part in rate
                ]
            )
            m_re, m_im = in_map[d, 0], in_map[d, 1]
            f_re, f_im = factor_re[:, None, :], factor_im[:, None, :]
            enter = (
                (f_re * m_re - f_im * m_im).reshape(width, st),
                (f_re * m_im + f_im * m_re).reshape(width, st),
            )
            for which, q, chan, column, lanes in packs:
                if which != s:
                    continue
                for part in range(2):
                    push[d, part, :, column : column + lanes] = dot(
                        scaled[d, :, chan : chan + LANES],
                        spread(enter[part][q * LANES : (q + 1) * LANES], masks[s]),
                    )
    rate_all = [
        [jnp.concatenate([rates[d][0][part], rates[d][1][part]], axis=1) for part in range(2)]
        for d in range(2)
    ]

    for _, _, _, column, lanes in packs:
        cols = slice(column, column + lanes)
        for d in range(2):
            r_re, r_im = rate_all[d][0][:, cols], rate_all[d][1][:, cols]
            h_re = h_im = None
            for step in steps_of(steps, d):
                at = slice(step * SUB, (step + 1) * SUB)
                p_re, p_im = push[d, 0, at, cols], push[d, 1, at, cols]
                if h_re is None:
                    h_re, h_im = p_re, p_im
                else:
                    h_re, h_im = r_re * h_re - r_im * h_im + p_re, r_re * h_im + r_im * h_re + p_im
            ends[d, 0, :, cols] = h_re
            ends[d, 1, :, cols] = h_im

    sub = iota((SUB, total), 0)
    message, powers = [], []
    folds = total // LANES

    def fold(value):
        return jnp.concatenate([value[:, i * LANES : (i + 1) * LANES] for i in range(folds)], axis=0)
    for d in range(2):
        power = tuple(rate_all[d])
        taken = 1
        while taken < steps:
            power = square(*power)
            taken *= 2
        a = (power[0] * kept[d], power[1] * kept[d])
        b = (ends[d, 0] * kept[d], ends[d, 1] * kept[d])

        def moved(value, by, fill):
            shift = by if d == 0 else SUB - by
            fine = sub >= by if d == 0 else sub < SUB - by
            return jnp.where(fine, pltpu.roll(value, shift, 0), fill)

        by = 1
        while by < SUB:
            pa = (moved(a[0], by, 1.0), moved(a[1], by, 0.0))
            pb = (moved(b[0], by, 0.0), moved(b[1], by, 0.0))
            b = plus(times(a, pb), b)
            a = times(a, pa)
            by *= 2
        before[d, 0] = moved(a[0], 1, 1.0)
        before[d, 1] = moved(a[1], 1, 0.0)
        before[d, 2] = moved(b[0], 1, 0.0)
        before[d, 3] = moved(b[1], 1, 0.0)
        edge = slice(SUB - 1, SUB) if d == 0 else slice(0, 1)
        message.append((fold(kept_all[d]), (fold(b[0][edge]), fold(b[1][edge]))))
        stride_power = tuple(fold(part) for part in rate_all[d])
        taken = 1
        while taken < tokens:
            stride_power = square(*stride_power)
            taken *= 2
        powers.append(stride_power)

    pl.semaphore_wait(barrier, 3 * (SIDE - 1) + 1)
    carry = [None, None]
    scan_copies = []
    for stage in range(3):
        stride = SIDE**stage
        place = lax.rem(sp // stride, SIDE)
        block = jnp.concatenate([part for k, b in message for part in (k, b[0], b[1])], axis=0)
        msg[stage] = block.astype(BF16)
        copies = []
        for k in range(1, SIDE):
            there = lax.rem(place + k, SIDE)
            copy = pltpu.make_async_remote_copy(
                src_ref=msg.at[stage],
                dst_ref=recv_ends.at[stage, place],
                send_sem=scan_send.at[stage * SIDE + k],
                recv_sem=scan_recv.at[stage * SIDE + k],
                device_id={"sp": sp + (there - place) * stride, "tp": tp},
                device_id_type=MESH,
            )
            copy.start()
            copies.append(copy)
        recv_ends[stage, place] = block.astype(BF16)
        if stage < 2:
            fetches[2 + stage].start()
        if stage == 0:
            for small in smalls[8:]:
                small.wait()
            for s in range(2):
                for d in range(2):
                    for part in range(2):
                        rows = sets[s][3][d, part].reshape(width, states_of[s])
                        if part:
                            rows = -rows
                        for which, q, _, column, lanes in packs:
                            if which == s:
                                begin = 2 * column + part * lanes
                                leave[d, :, begin : begin + lanes] = spread(
                                    rows[q * LANES : (q + 1) * LANES], masks[s]
                                )
                gate_rows = gate_mix[s].astype(F32).reshape(width, channels)
                gate_mask = (iota((LANES, LANES), 0) // channels) == (iota((LANES, LANES), 1) // channels)
                for q in range(groups // per):
                    gates[s * (groups // per) + q] = spread(
                        gate_rows[q * LANES : (q + 1) * LANES], gate_mask
                    )
        for copy in copies:
            copy.wait_recv()
        scan_copies += copies
        fetched = [recv_ends[stage, j].astype(F32) for j in range(SIDE)]
        for d in range(2):
            one = jnp.ones((folds, LANES), F32)
            zero = jnp.zeros((folds, LANES), F32)
            pre_a, pre_b = (one, zero), (zero, zero)
            run_a, tot_k, tot_b = None, None, None
            for j in steps_of(SIDE, d):
                use = (j < place) if d == 0 else (j > place)
                begin = 3 * d * folds
                k, b_re, b_im = (fetched[j][begin + r * folds : begin + (r + 1) * folds] for r in range(3))
                a, b = (powers[d][0] * k, powers[d][1] * k), (b_re, b_im)
                if tot_b is None:
                    run_a, tot_k, tot_b = a, k, b
                else:
                    run_a, tot_k, tot_b = times(a, run_a), k * tot_k, plus(times(a, tot_b), b)
                pre_a = tuple(jnp.where(use, new, old) for new, old in zip(run_a, pre_a))
                pre_b = tuple(jnp.where(use, new, old) for new, old in zip(tot_b, pre_b))
            message[d] = (tot_k, tot_b)
            powers[d] = square(*square(*powers[d]))
            if carry[d] is None:
                carry[d] = (pre_a, pre_b)
            else:
                carry[d] = (times(carry[d][0], pre_a), plus(times(carry[d][0], pre_b), carry[d][1]))

    for d in range(2):
        c_re, c_im = (
            jnp.concatenate([part[i : i + 1] for i in range(folds)], axis=1) for part in carry[d][1]
        )
        a_re, a_im = before[d, 0], before[d, 1]
        ends[d, 0] = a_re * c_re - a_im * c_im + before[d, 2]
        ends[d, 1] = a_re * c_im + a_im * c_re + before[d, 3]

    for index, (s, q, chan, column, lanes) in enumerate(packs):
        cols = slice(column, column + lanes)
        chans = slice(chan, chan + LANES)
        read = skip[s : s + 1, q * LANES : (q + 1) * LANES].astype(F32) * plain[:, chans]
        for d in range(2):
            r_re, r_im = rate_all[d][0][:, cols], rate_all[d][1][:, cols]
            h_re, h_im = ends[d, 0, :, cols], ends[d, 1, :, cols]
            held = None
            for step in steps_of(steps, d):
                at = slice(step * SUB, (step + 1) * SUB)
                p_re, p_im = push[d, 0, at, cols], push[d, 1, at, cols]
                h_re, h_im = r_re * h_re - r_im * h_im + p_re, r_re * h_im + r_im * h_re + p_im
                if held is None:
                    held = (h_re, h_im)
                else:
                    low = min(step, step + 1 if d else step - 1) * SUB
                    for part, new in enumerate((h_re, h_im)):
                        both = [held[part], new] if d == 0 else [new, held[part]]
                        states[d, low : low + 2 * SUB, part * lanes : (part + 1) * lanes] = (
                            jnp.concatenate(both, axis=0).astype(BF16)
                        )
                    held = None
            term = dot(
                states[d, :, : 2 * lanes], leave[d, :, 2 * column : 2 * column + 2 * lanes], ((1,), (1,))
            )
            read = read + shrink[d, :, chans] * term
        active = jax.nn.gelu(read, approximate=True)
        opened = jax.nn.sigmoid(dot(active.astype(BF16), gates[index]))
        woven[:, chans] = (active * opened).astype(BF16)

    half = tokens // 2
    halves[...] = dot(unweave, woven[...]).astype(BF16).reshape(halves.shape)
    swap = pltpu.make_async_remote_copy(
        src_ref=halves.at[1 - tp],
        dst_ref=pair.at[tp],
        send_sem=pair_sem.at[0],
        recv_sem=pair_sem.at[1],
        device_id={"sp": sp, "tp": 1 - tp},
        device_id_type=MESH,
    )
    swap.start()
    pair[tp] = halves[tp]

    def partner(k, flip, sign):
        m = lax.rem(k, n_sp // 2)
        dz, dy = m // (2 * SIDE), lax.rem(m // 2, SIDE)
        dx = 2 * lax.rem(m, 2) + lax.rem(dz + dy + k // (n_sp // 2), 2)
        z, y, x = sp // (SIDE * SIDE), lax.rem(sp // SIDE, SIDE), lax.rem(sp, SIDE)
        z, y, x = (lax.rem(at + sign * by + SIDE, SIDE) for at, by in ((z, dz), (y, dy), (x, dx)))
        return z * SIDE * SIDE + y * SIDE + x, (tp if flip == 0 else 1 - tp)

    upper = ones_where(iota((half, half), 0) < iota((half, half), 1), BF16)
    share_sum = route_weights[0:1, :] + route_weights[1:2, :]
    line = iota((2 * n_sp, half), 0)
    slot = lax.rem(line, 2).astype(F32)
    spots, highs, lows = [], [], []
    for flip in range(2):
        other, side = partner(line // 2, flip, 1)
        picks = other * 2 + side
        named = [routes[k : k + 1, :] == picks for k in range(2)]
        any_named = ones_where(named[0] | named[1])
        chosen = dot(any_named.astype(BF16), upper) == slot
        spots.append(jnp.where(chosen, any_named, 0.0).astype(BF16))
        weight = sum(
            jnp.where(named[k] & chosen, route_weights[k : k + 1, :] / share_sum, 0.0) for k in range(2)
        )
        highs.append(weight.astype(BF16))
        lows.append((weight - highs[flip].astype(F32)).astype(BF16))
    fetches[0].wait()
    swap.wait_recv()
    joined = jnp.concatenate(
        [pair[k, :, :width] for k in range(2)] + [pair[k, :, width:] for k in range(2)], axis=1
    ).astype(F32)
    scale = lax.rsqrt(jnp.mean(joined * joined, axis=1, keepdims=True) + epsilon)
    mixed = (joined * scale * mixer_gain[...]).astype(BF16)
    hidden1 = (residual[...].astype(F32) + dot(mixed, proj_v[...])).astype(BF16)
    hidden_wide = hidden1.astype(F32)
    normed = (
        hidden_wide
        * lax.rsqrt(jnp.mean(hidden_wide * hidden_wide, axis=1, keepdims=True) + epsilon)
        * ffn_gain[...]
    ).astype(BF16)
    for flip in range(2):
        sec[flip] = dot(spots[flip], normed).astype(BF16).reshape(sec.shape[1:])
        if flip == 0:
            own = pltpu.make_async_copy(sec.at[0, 0], arrived.at[0, 0], self_sem.at[0])
            own.start()

        def send(k, _):
            k = n_sp - 1 - k if flip else n_sp - k
            other, side = partner(k, flip, 1)
            pltpu.make_async_remote_copy(
                src_ref=sec.at[flip, k],
                dst_ref=arrived.at[flip, k],
                send_sem=send_sem.at[flip],
                recv_sem=recv_sem.at[flip],
                device_id={"sp": other, "tp": side},
                device_id_type=MESH,
            ).start()
            return 0

        lax.fori_loop(1 - flip, n_sp, send, 0)

    own.wait()
    for fetch in fetches[1:]:
        fetch.wait()
    def wait_bytes(ref, count, sem):
        pltpu.make_async_copy(ref.at[pl.ds(0, count)], ref.at[pl.ds(0, count)], sem).wait()

    for flip in range(2):
        wait_bytes(arrived.at[flip], n_sp - 1 + flip, recv_sem.at[flip])
        rows_v[...] = arrived[flip].reshape(rows_v.shape)

        gate_val = dot(rows_v[...], gate_v[...])
        up_val = dot(rows_v[...], up_v[...])
        hidden_v[...] = (jax.nn.silu(gate_val) * up_val).astype(BF16)
        served[flip] = dot(hidden_v[...], down_v[...]).astype(BF16).reshape(served.shape[1:])

        def give(k, _):
            k = n_sp - 1 - k if flip else n_sp - k
            other, side = partner(k, flip, -1)
            pltpu.make_async_remote_copy(
                src_ref=served.at[flip, k],
                dst_ref=returned.at[flip, k],
                send_sem=back_send.at[flip],
                recv_sem=back_recv.at[flip],
                device_id={"sp": other, "tp": side},
                device_id_type=MESH,
            ).start()
            return 0

        lax.fori_loop(1 - flip, n_sp, give, 0)
        if flip == 0:
            own_back = pltpu.make_async_copy(served.at[0, 0], returned.at[0, 0], self_sem.at[1])
            own_back.start()

    own_back.wait()
    result = hidden_wide
    for flip in range(2):
        wait_bytes(returned.at[flip], n_sp - 1 + flip, back_recv.at[flip])
        back = returned[flip].reshape(2 * n_sp, -1)
        result = result + dot(highs[flip], back, ((0,), (0,))) + dot(lows[flip], back, ((0,), (0,)))
    out_ref[...] = result.astype(BF16)

    for copy in scan_copies:
        copy.wait_send()
    swap.wait_send()
    for flip in range(2):
        wait_bytes(sec.at[flip], n_sp - 1 + flip, send_sem.at[flip])
        wait_bytes(served.at[flip], n_sp - 1 + flip, back_send.at[flip])


def local(
    wide_inputs, narrow_inputs, wide_poles, narrow_poles, step_sizes, forget, wide_in_map,
    narrow_in_map, wide_out_map, narrow_out_map, skip_weight, gate_mix, residual, mixer_gain,
    out_proj, ffn_gain, routes, route_weights, gate_proj, up_proj, down_proj,
):
    n_sp = lax.axis_size("sp")
    tokens, width = wide_inputs.shape
    groups = wide_in_map.shape[2]
    total = groups * (wide_in_map.shape[4] + narrow_in_map.shape[4])
    widest = LANES // wide_in_map.shape[3] * wide_in_map.shape[4]
    rows, model = residual.shape
    fe = gate_proj.shape[2]
    hbm = pl.BlockSpec(memory_space=pltpu.HBM)
    smalls = (
        wide_inputs, narrow_inputs, forget, wide_poles, narrow_poles, step_sizes, wide_in_map,
        narrow_in_map, wide_out_map, narrow_out_map, gate_mix, skip_weight, routes.T,
        route_weights.T, mixer_gain.reshape(1, -1), ffn_gain.reshape(1, -1), residual,
    )
    dma = pltpu.SemaphoreType.DMA
    result = pl.pallas_call(
        layer_kernel,
        out_shape=jax.ShapeDtypeStruct((rows, model), BF16),
        in_specs=[hbm] * (SMALL + 4),
        out_specs=pl.BlockSpec(memory_space=pltpu.VMEM),
        scratch_shapes=[pltpu.VMEM(each.shape, each.dtype) for each in smalls]
        + [
            pltpu.VMEM(out_proj.shape, BF16),
            pltpu.VMEM((model, fe), BF16),
            pltpu.VMEM((model, fe), BF16),
            pltpu.VMEM((fe, model), BF16),
            pltpu.VMEM((2, 2, tokens, total), F32),
            pltpu.VMEM((2, tokens, 2 * width), BF16),
            pltpu.VMEM((2, tokens, 2 * width), F32),
            pltpu.VMEM((tokens, 2 * width), F32),
            pltpu.VMEM((2, LANES, 2 * total), BF16),
            pltpu.VMEM((2 * width // LANES, LANES, LANES), BF16),
            pltpu.VMEM((2, 2, SUB, total), F32),
            pltpu.VMEM((2, 4, SUB, total), F32),
            pltpu.VMEM((3, SIDE, 6 * total // LANES, LANES), BF16),
            pltpu.VMEM((3, 6 * total // LANES, LANES), BF16),
            pltpu.VMEM((2, tokens, 2 * widest), BF16),
            pltpu.VMEM((tokens, 2 * width), BF16),
            pltpu.VMEM((2, tokens // 2, 2 * width), BF16),
            pltpu.VMEM((2, tokens // 2, 2 * width), BF16),
            pltpu.VMEM((2, n_sp, 2, model), BF16),
            pltpu.VMEM((2, n_sp, 2, model), BF16),
            pltpu.VMEM((2 * n_sp, model), BF16),
            pltpu.VMEM((2 * n_sp, fe), BF16),
            pltpu.VMEM((2, n_sp, 2, model), BF16),
            pltpu.VMEM((2, n_sp, 2, model), BF16),
            dma((4,)), dma((3 * SIDE,)), dma((3 * SIDE,)), dma((2,)), dma((2,)), dma((2,)), dma((2,)),
            dma((2,)), dma((2,)), dma((SMALL,)),
        ],
        compiler_params=pltpu.CompilerParams(
            collective_id=0, has_side_effects=True, vmem_limit_bytes=60 * 1024 * 1024
        ),
        name="layer",
    )(*smalls, out_proj, gate_proj, up_proj, down_proj)
    return result


def solution(mesh):
    return jax.shard_map(
        local,
        mesh=mesh,
        in_specs=(
            P("sp", "tp"),
            P("sp", "tp"),
            P(None, None, "tp", None),
            P(None, None, "tp", None),
            P(None, None, "tp"),
            P(None, None, "tp", "sp"),
            P(None, None, "tp", None, None),
            P(None, None, "tp", None, None),
            P(None, None, "tp", None, None),
            P(None, None, "tp", None, None),
            P(None, "tp"),
            P(None, "tp", None, None),
            P(("sp", "tp"), None),
            P(),
            P(),
            P(),
            P(("sp", "tp"), None),
            P(("sp", "tp"), None),
            P(("sp", "tp"), None, None),
            P(("sp", "tp"), None, None),
            P(("sp", "tp"), None, None),
        ),
        out_specs=P(("sp", "tp"), None),
        check_vma=False,
    )
```

```python
import functools

import jax
import jax.numpy as jnp
from jax import lax
from jax.experimental import pallas as pl
from jax.experimental.pallas import tpu as pltpu
from jax.sharding import PartitionSpec as P

epsilon = 1e-06
SIDE = 4
SUB = 8
SMALL = 17
LANES = 128
EXACT = lax.Precision.HIGHEST
F32 = jnp.float32
BF16 = jnp.bfloat16
MESH = pl.DeviceIdType.MESH


def iota(shape, dim):
    return lax.broadcasted_iota(jnp.int32, shape, dim)


def ones_where(mask, dtype=F32):
    return jnp.where(mask, 1.0, 0.0).astype(dtype)


def dot(a, b, contract=((1,), (0,)), precision=None):
    return lax.dot_general(a, b, (contract, ((), ())), precision=precision, preferred_element_type=F32)


def sine_cosine(angle):
    y = angle * 0.25
    q = y * y
    s = y * (1.0 + q * (-1 / 6 + q * (1 / 120 + q * (-1 / 5040 + q * (1 / 362880)))))
    c = 1.0 + q * (-0.5 + q * (1 / 24 + q * (-1 / 720 + q * (1 / 40320 + q * (-1 / 3628800)))))
    for _ in range(2):
        s, c = 2.0 * s * c, 1.0 - 2.0 * s * s
    return s, c


def square(re, im):
    return re * re - im * im, 2.0 * re * im


def times(a, b):
    return a[0] * b[0] - a[1] * b[1], a[0] * b[1] + a[1] * b[0]


def plus(a, b):
    return a[0] + b[0], a[1] + b[1]


def spread(rows, mask):
    copies = mask.shape[1] // rows.shape[1]
    tiled = jnp.concatenate([rows] * copies, axis=1)
    return jnp.where(mask, tiled, 0.0).astype(BF16)


def steps_of(count, direction):
    return range(count) if direction == 0 else range(count - 1, -1, -1)


def layer_kernel(*refs):
    sources, refs = refs[:SMALL], refs[SMALL:]
    (out_proj, gate_proj, up_proj, down_proj, out_ref), refs = refs[:5], refs[5:]
    staged, refs = refs[:SMALL], refs[SMALL:]
    layer_body(sources, staged, out_proj, gate_proj, up_proj, down_proj, out_ref, *refs)


def layer_body(
    sources, staged, out_proj, gate_proj, up_proj, down_proj, out_ref,
    proj_v, gate_v, up_v, down_v, push, scaled, shrink, plain, leave, gates, ends, before, recv_ends,
    msg, states, woven, halves, pair, sec, arrived, rows_v, hidden_v, served, returned,
    weight_sem, scan_send, scan_recv, pair_sem, send_sem, recv_sem, back_send, back_recv, self_sem, small_sem,
):
    (
        wide_u, narrow_u, forget, wide_poles, narrow_poles, step_sizes, wide_in, narrow_in, wide_out,
        narrow_out, gate_mix, skip, routes, route_weights, mixer_gain, ffn_gain, residual,
    ) = staged
    smalls = [
        pltpu.make_async_copy(source, target, small_sem.at[i])
        for i, (source, target) in enumerate(zip(sources, staged))
    ]
    for small in smalls:
        small.start()
    n_sp = lax.axis_size("sp")
    sp = lax.axis_index("sp")
    tp = lax.axis_index("tp")

    barrier = pltpu.get_barrier_semaphore()

    for stage in range(3):
        stride = SIDE**stage
        place = lax.rem(sp // stride, SIDE)
        for k in range(1, SIDE):
            there = lax.rem(place + k, SIDE)
            pl.semaphore_signal(
                barrier,
                inc=1,
                device_id={"sp": sp + (there - place) * stride, "tp": tp},
                device_id_type=MESH,
            )
    pl.semaphore_signal(barrier, inc=1, device_id={"sp": sp, "tp": 1 - tp}, device_id_type=MESH)
    fetches = [
        pltpu.make_async_copy(source, target, weight_sem.at[i])
        for i, (source, target) in enumerate(
            ((out_proj, proj_v), (gate_proj.at[0], gate_v), (up_proj.at[0], up_v), (down_proj.at[0], down_v))
        )
    ]
    for fetch in fetches[:2]:
        fetch.start()

    for small in smalls[:8]:
        small.wait()
    tokens = wide_u.shape[0]
    steps = tokens // SUB
    sets = (
        (wide_u, wide_poles, wide_in, wide_out),
        (narrow_u, narrow_poles, narrow_in, narrow_out),
    )
    groups, channels = wide_in.shape[2], wide_in.shape[3]
    width = groups * channels
    per = LANES // channels
    states_of = [each[2].shape[4] for each in sets]
    bases = [0, groups * states_of[0]]
    total = groups * sum(states_of)
    packs = []
    for s in range(2):
        for q in range(groups // per):
            packs.append((s, q, s * width + q * LANES, bases[s] + q * per * states_of[s], per * states_of[s]))

    row = iota((tokens, tokens), 0)
    col = iota((tokens, tokens), 1)
    weave = ones_where(col == lax.rem(row, SUB) * steps + row // SUB, BF16)
    unweave = ones_where(col == lax.rem(row, steps) * SUB + row // steps, BF16)
    same = (col // steps) == lax.rem(row, SUB)
    reach = (
        ones_where(same & (lax.rem(col, steps) <= row // SUB)),
        ones_where(same & (lax.rem(col, steps) >= row // SUB)),
    )
    for s in range(2):
        plain[:, s * width : (s + 1) * width] = dot(weave, sets[s][0][...])
    to_channel = ones_where(iota((2 * groups, 2 * width), 0) == iota((2 * groups, 2 * width), 1) // channels)
    lane = iota((2 * groups, total), 1)
    owner = jnp.where(
        lane < bases[1], lane // states_of[0], groups + (lane - bases[1]) // states_of[1]
    )
    to_lane = ones_where(iota((2 * groups, total), 0) == owner)
    kept, kept_all = [], []
    for d in range(2):
        flat = forget[d].reshape(2 * groups, tokens)
        lost = dot(reach[d], flat, ((1,), (1,)), EXACT)
        wide = dot(lost, to_channel, precision=EXACT)
        shrink[d] = jnp.exp(-wide)
        scaled[d] = (plain[...] * jnp.exp(wide)).astype(BF16)
        last = lost[tokens - SUB :] if d == 0 else lost[:SUB]
        fall = dot(last, to_lane, precision=EXACT)
        kept.append(jnp.exp(-fall))
        kept_all.append(jnp.exp(-jnp.sum(fall, axis=0, keepdims=True)))

    masks = [
        (iota((LANES, per * st), 0) // channels) == (iota((LANES, per * st), 1) // st) for st in states_of
    ]
    eye = iota((groups, groups), 0) == iota((groups, groups), 1)
    rates = [[], []]
    for s in range(2):
        _, poles, in_map, out_map = sets[s]
        st = states_of[s]
        for d in range(2):
            re, im = poles[d, 0], poles[d, 1]
            growth = jnp.exp(re)
            sine, cosine = sine_cosine(im)
            rate = (growth * cosine, growth * sine)
            numer_re, numer_im = rate[0] - 1.0, rate[1]
            step = jnp.sum(jnp.where(eye, step_sizes[d, s : s + 1, :], 0.0), axis=1, keepdims=True)
            over = step / (re * re + im * im)
            factor_re = (numer_re * re + numer_im * im) * over
            factor_im = (numer_im * re - numer_re * im) * over
            flat_mask = iota((groups, groups * st), 0) == iota((groups, groups * st), 1) // st
            rates[d].append(
                [
                    jnp.sum(
                        jnp.where(flat_mask, jnp.concatenate([part] * groups, axis=1), 0.0),
                        axis=0,
                        keepdims=True,
                    )
                    for part in rate
                ]
            )
            m_re, m_im = in_map[d, 0], in_map[d, 1]
            f_re, f_im = factor_re[:, None, :], factor_im[:, None, :]
            enter = (
                (f_re * m_re - f_im * m_im).reshape(width, st),
                (f_re * m_im + f_im * m_re).reshape(width, st),
            )
            for which, q, chan, column, lanes in packs:
                if which != s:
                    continue
                for part in range(2):
                    push[d, part, :, column : column + lanes] = dot(
                        scaled[d, :, chan : chan + LANES],
                        spread(enter[part][q * LANES : (q + 1) * LANES], masks[s]),
                    )
    rate_all = [
        [jnp.concatenate([rates[d][0][part], rates[d][1][part]], axis=1) for part in range(2)]
        for d in range(2)
    ]

    for _, _, _, column, lanes in packs:
        cols = slice(column, column + lanes)
        for d in range(2):
            r_re, r_im = rate_all[d][0][:, cols], rate_all[d][1][:, cols]
            h_re = h_im = None
            for step in steps_of(steps, d):
                at = slice(step * SUB, (step + 1) * SUB)
                p_re, p_im = push[d, 0, at, cols], push[d, 1, at, cols]
                if h_re is None:
                    h_re, h_im = p_re, p_im
                else:
                    h_re, h_im = r_re * h_re - r_im * h_im + p_re, r_re * h_im + r_im * h_re + p_im
            ends[d, 0, :, cols] = h_re
            ends[d, 1, :, cols] = h_im

    sub = iota((SUB, total), 0)
    message, powers = [], []
    folds = total // LANES

    def fold(value):
        return jnp.concatenate([value[:, i * LANES : (i + 1) * LANES] for i in range(folds)], axis=0)
    for d in range(2):
        power = tuple(rate_all[d])
        taken = 1
        while taken < steps:
            power = square(*power)
            taken *= 2
        a = (power[0] * kept[d], power[1] * kept[d])
        b = (ends[d, 0] * kept[d], ends[d, 1] * kept[d])

        def moved(value, by, fill):
            shift = by if d == 0 else SUB - by
            fine = sub >= by if d == 0 else sub < SUB - by
            return jnp.where(fine, pltpu.roll(value, shift, 0), fill)

        by = 1
        while by < SUB:
            pa = (moved(a[0], by, 1.0), moved(a[1], by, 0.0))
            pb = (moved(b[0], by, 0.0), moved(b[1], by, 0.0))
            b = plus(times(a, pb), b)
            a = times(a, pa)
            by *= 2
        before[d, 0] = moved(a[0], 1, 1.0)
        before[d, 1] = moved(a[1], 1, 0.0)
        before[d, 2] = moved(b[0], 1, 0.0)
        before[d, 3] = moved(b[1], 1, 0.0)
        edge = slice(SUB - 1, SUB) if d == 0 else slice(0, 1)
        message.append((fold(kept_all[d]), (fold(b[0][edge]), fold(b[1][edge]))))
        stride_power = tuple(fold(part) for part in rate_all[d])
        taken = 1
        while taken < tokens:
            stride_power = square(*stride_power)
            taken *= 2
        powers.append(stride_power)

    pl.semaphore_wait(barrier, 3 * (SIDE - 1) + 1)
    carry = [None, None]
    scan_copies = []
    for stage in range(3):
        stride = SIDE**stage
        place = lax.rem(sp // stride, SIDE)
        block = jnp.concatenate([part for k, b in message for part in (k, b[0], b[1])], axis=0)
        msg[stage] = block.astype(BF16)
        copies = []
        for k in range(1, SIDE):
            there = lax.rem(place + k, SIDE)
            copy = pltpu.make_async_remote_copy(
                src_ref=msg.at[stage],
                dst_ref=recv_ends.at[stage, place],
                send_sem=scan_send.at[stage * SIDE + k],
                recv_sem=scan_recv.at[stage * SIDE + k],
                device_id={"sp": sp + (there - place) * stride, "tp": tp},
                device_id_type=MESH,
            )
            copy.start()
            copies.append(copy)
        recv_ends[stage, place] = block.astype(BF16)
        if stage < 2:
            fetches[2 + stage].start()
        if stage == 0:
            for small in smalls[8:]:
                small.wait()
            for s in range(2):
                for d in range(2):
                    for part in range(2):
                        rows = sets[s][3][d, part].reshape(width, states_of[s])
                        if part:
                            rows = -rows
                        for which, q, _, column, lanes in packs:
                            if which == s:
                                begin = 2 * column + part * lanes
                                leave[d, :, begin : begin + lanes] = spread(
                                    rows[q * LANES : (q + 1) * LANES], masks[s]
                                )
                gate_rows = gate_mix[s].astype(F32).reshape(width, channels)
                gate_mask = (iota((LANES, LANES), 0) // channels) == (iota((LANES, LANES), 1) // channels)
                for q in range(groups // per):
                    gates[s * (groups // per) + q] = spread(
                        gate_rows[q * LANES : (q + 1) * LANES], gate_mask
                    )
        for copy in copies:
            copy.wait_recv()
        scan_copies += copies
        fetched = [recv_ends[stage, j].astype(F32) for j in range(SIDE)]
        for d in range(2):
            one = jnp.ones((folds, LANES), F32)
            zero = jnp.zeros((folds, LANES), F32)
            pre_a, pre_b = (one, zero), (zero, zero)
            run_a, tot_k, tot_b = None, None, None
            for j in steps_of(SIDE, d):
                use = (j < place) if d == 0 else (j > place)
                begin = 3 * d * folds
                k, b_re, b_im = (fetched[j][begin + r * folds : begin + (r + 1) * folds] for r in range(3))
                a, b = (powers[d][0] * k, powers[d][1] * k), (b_re, b_im)
                if tot_b is None:
                    run_a, tot_k, tot_b = a, k, b
                else:
                    run_a, tot_k, tot_b = times(a, run_a), k * tot_k, plus(times(a, tot_b), b)
                pre_a = tuple(jnp.where(use, new, old) for new, old in zip(run_a, pre_a))
                pre_b = tuple(jnp.where(use, new, old) for new, old in zip(tot_b, pre_b))
            message[d] = (tot_k, tot_b)
            powers[d] = square(*square(*powers[d]))
            if carry[d] is None:
                carry[d] = (pre_a, pre_b)
            else:
                carry[d] = (times(carry[d][0], pre_a), plus(times(carry[d][0], pre_b), carry[d][1]))

    for d in range(2):
        c_re, c_im = (
            jnp.concatenate([part[i : i + 1] for i in range(folds)], axis=1) for part in carry[d][1]
        )
        a_re, a_im = before[d, 0], before[d, 1]
        ends[d, 0] = a_re * c_re - a_im * c_im + before[d, 2]
        ends[d, 1] = a_re * c_im + a_im * c_re + before[d, 3]

    for index, (s, q, chan, column, lanes) in enumerate(packs):
        cols = slice(column, column + lanes)
        chans = slice(chan, chan + LANES)
        read = skip[s : s + 1, q * LANES : (q + 1) * LANES].astype(F32) * plain[:, chans]
        for d in range(2):
            r_re, r_im = rate_all[d][0][:, cols], rate_all[d][1][:, cols]
            h_re, h_im = ends[d, 0, :, cols], ends[d, 1, :, cols]
            held = None
            for step in steps_of(steps, d):
                at = slice(step * SUB, (step + 1) * SUB)
                p_re, p_im = push[d, 0, at, cols], push[d, 1, at, cols]
                h_re, h_im = r_re * h_re - r_im * h_im + p_re, r_re * h_im + r_im * h_re + p_im
                if held is None:
                    held = (h_re, h_im)
                else:
                    low = min(step, step + 1 if d else step - 1) * SUB
                    for part, new in enumerate((h_re, h_im)):
                        both = [held[part], new] if d == 0 else [new, held[part]]
                        states[d, low : low + 2 * SUB, part * lanes : (part + 1) * lanes] = (
                            jnp.concatenate(both, axis=0).astype(BF16)
                        )
                    held = None
            term = dot(
                states[d, :, : 2 * lanes], leave[d, :, 2 * column : 2 * column + 2 * lanes], ((1,), (1,))
            )
            read = read + shrink[d, :, chans] * term
        active = jax.nn.gelu(read, approximate=True)
        opened = jax.nn.sigmoid(dot(active.astype(BF16), gates[index]))
        woven[:, chans] = (active * opened).astype(BF16)

    half = tokens // 2
    halves[...] = dot(unweave, woven[...]).astype(BF16).reshape(halves.shape)
    swap = pltpu.make_async_remote_copy(
        src_ref=halves.at[1 - tp],
        dst_ref=pair.at[tp],
        send_sem=pair_sem.at[0],
        recv_sem=pair_sem.at[1],
        device_id={"sp": sp, "tp": 1 - tp},
        device_id_type=MESH,
    )
    swap.start()

    def partner(k, flip, sign):
        m = lax.rem(k, n_sp // 2)
        dz, dy = m // (2 * SIDE), lax.rem(m // 2, SIDE)
        dx = 2 * lax.rem(m, 2) + lax.rem(dz + dy + k // (n_sp // 2), 2)
        z, y, x = sp // (SIDE * SIDE), lax.rem(sp // SIDE, SIDE), lax.rem(sp, SIDE)
        z, y, x = (lax.rem(at + sign * by + SIDE, SIDE) for at, by in ((z, dz), (y, dy), (x, dx)))
        return z * SIDE * SIDE + y * SIDE + x, (tp if flip == 0 else 1 - tp)

    upper = ones_where(iota((half, half), 0) < iota((half, half), 1), BF16)
    share_sum = route_weights[0:1, :] + route_weights[1:2, :]
    line = iota((2 * n_sp, half), 0)
    slot = lax.rem(line, 2).astype(F32)
    spots, highs, lows = [], [], []
    for flip in range(2):
        other, side = partner(line // 2, flip, 1)
        picks = other * 2 + side
        named = [routes[k : k + 1, :] == picks for k in range(2)]
        any_named = ones_where(named[0] | named[1])
        chosen = dot(any_named.astype(BF16), upper) == slot
        spots.append(jnp.where(chosen, any_named, 0.0).astype(BF16))
        weight = sum(
            jnp.where(named[k] & chosen, route_weights[k : k + 1, :] / share_sum, 0.0) for k in range(2)
        )
        highs.append(weight.astype(BF16))
        lows.append((weight - highs[flip].astype(F32)).astype(BF16))
    fetches[0].wait()

    def projected(side, block):
        wide = pl.ds(pl.multiple_of(side * width, width), width)
        narrow = pl.ds(pl.multiple_of((2 + side) * width, width), width)
        values = block.astype(F32)
        gain = jnp.concatenate([mixer_gain[:, wide], mixer_gain[:, narrow]], axis=1)
        scaled_by = (values * gain).astype(BF16)
        product = dot(scaled_by[:, :width], proj_v[wide, :]) + dot(scaled_by[:, width:], proj_v[narrow, :])
        return product, jnp.sum(values * values, axis=1, keepdims=True)

    own_product, own_square = projected(tp, halves[tp])
    swap.wait_recv()
    their_product, their_square = projected(1 - tp, pair[1 - tp])
    scale = lax.rsqrt((own_square + their_square) / (4 * width) + epsilon)
    product = (own_product + their_product) * scale
    hidden1 = (residual[...].astype(F32) + product).astype(BF16)
    hidden_wide = hidden1.astype(F32)
    normed = (
        hidden_wide
        * lax.rsqrt(jnp.mean(hidden_wide * hidden_wide, axis=1, keepdims=True) + epsilon)
        * ffn_gain[...]
    ).astype(BF16)
    for flip in range(2):
        sec[flip] = dot(spots[flip], normed).astype(BF16).reshape(sec.shape[1:])
        if flip == 0:
            own = pltpu.make_async_copy(sec.at[0, 0], arrived.at[0, 0], self_sem.at[0])
            own.start()

        def send(k, _):
            k = n_sp - 1 - k if flip else n_sp - k
            other, side = partner(k, flip, 1)
            pltpu.make_async_remote_copy(
                src_ref=sec.at[flip, k],
                dst_ref=arrived.at[flip, k],
                send_sem=send_sem.at[flip],
                recv_sem=recv_sem.at[flip],
                device_id={"sp": other, "tp": side},
                device_id_type=MESH,
            ).start()
            return 0

        lax.fori_loop(1 - flip, n_sp, send, 0)

    own.wait()
    for fetch in fetches[1:]:
        fetch.wait()
    def wait_bytes(ref, count, sem):
        pltpu.make_async_copy(ref.at[pl.ds(0, count)], ref.at[pl.ds(0, count)], sem).wait()

    for flip in range(2):
        wait_bytes(arrived.at[flip], n_sp - 1 + flip, recv_sem.at[flip])
        rows_v[...] = arrived[flip].reshape(rows_v.shape)

        gate_val = dot(rows_v[...], gate_v[...])
        up_val = dot(rows_v[...], up_v[...])
        hidden_v[...] = (jax.nn.silu(gate_val) * up_val).astype(BF16)
        served[flip] = dot(hidden_v[...], down_v[...]).astype(BF16).reshape(served.shape[1:])

        def give(k, _):
            k = n_sp - 1 - k if flip else n_sp - k
            other, side = partner(k, flip, -1)
            pltpu.make_async_remote_copy(
                src_ref=served.at[flip, k],
                dst_ref=returned.at[flip, k],
                send_sem=back_send.at[flip],
                recv_sem=back_recv.at[flip],
                device_id={"sp": other, "tp": side},
                device_id_type=MESH,
            ).start()
            return 0

        lax.fori_loop(1 - flip, n_sp, give, 0)
        if flip == 0:
            own_back = pltpu.make_async_copy(served.at[0, 0], returned.at[0, 0], self_sem.at[1])
            own_back.start()

    own_back.wait()
    result = hidden_wide
    for flip in range(2):
        wait_bytes(returned.at[flip], n_sp - 1 + flip, back_recv.at[flip])
        back = returned[flip].reshape(2 * n_sp, -1)
        result = result + dot(highs[flip], back, ((0,), (0,))) + dot(lows[flip], back, ((0,), (0,)))
    out_ref[...] = result.astype(BF16)

    for copy in scan_copies:
        copy.wait_send()
    swap.wait_send()
    for flip in range(2):
        wait_bytes(sec.at[flip], n_sp - 1 + flip, send_sem.at[flip])
        wait_bytes(served.at[flip], n_sp - 1 + flip, back_send.at[flip])


def local(
    wide_inputs, narrow_inputs, wide_poles, narrow_poles, step_sizes, forget, wide_in_map,
    narrow_in_map, wide_out_map, narrow_out_map, skip_weight, gate_mix, residual, mixer_gain,
    out_proj, ffn_gain, routes, route_weights, gate_proj, up_proj, down_proj,
):
    n_sp = lax.axis_size("sp")
    tokens, width = wide_inputs.shape
    groups = wide_in_map.shape[2]
    total = groups * (wide_in_map.shape[4] + narrow_in_map.shape[4])
    widest = LANES // wide_in_map.shape[3] * wide_in_map.shape[4]
    rows, model = residual.shape
    fe = gate_proj.shape[2]
    hbm = pl.BlockSpec(memory_space=pltpu.HBM)
    smalls = (
        wide_inputs, narrow_inputs, forget, wide_poles, narrow_poles, step_sizes, wide_in_map,
        narrow_in_map, wide_out_map, narrow_out_map, gate_mix, skip_weight, routes.T,
        route_weights.T, mixer_gain.reshape(1, -1), ffn_gain.reshape(1, -1), residual,
    )
    dma = pltpu.SemaphoreType.DMA
    result = pl.pallas_call(
        layer_kernel,
        out_shape=jax.ShapeDtypeStruct((rows, model), BF16),
        in_specs=[hbm] * (SMALL + 4),
        out_specs=pl.BlockSpec(memory_space=pltpu.VMEM),
        scratch_shapes=[pltpu.VMEM(each.shape, each.dtype) for each in smalls]
        + [
            pltpu.VMEM(out_proj.shape, BF16),
            pltpu.VMEM((model, fe), BF16),
            pltpu.VMEM((model, fe), BF16),
            pltpu.VMEM((fe, model), BF16),
            pltpu.VMEM((2, 2, tokens, total), F32),
            pltpu.VMEM((2, tokens, 2 * width), BF16),
            pltpu.VMEM((2, tokens, 2 * width), F32),
            pltpu.VMEM((tokens, 2 * width), F32),
            pltpu.VMEM((2, LANES, 2 * total), BF16),
            pltpu.VMEM((2 * width // LANES, LANES, LANES), BF16),
            pltpu.VMEM((2, 2, SUB, total), F32),
            pltpu.VMEM((2, 4, SUB, total), F32),
            pltpu.VMEM((3, SIDE, 6 * total // LANES, LANES), BF16),
            pltpu.VMEM((3, 6 * total // LANES, LANES), BF16),
            pltpu.VMEM((2, tokens, 2 * widest), BF16),
            pltpu.VMEM((tokens, 2 * width), BF16),
            pltpu.VMEM((2, tokens // 2, 2 * width), BF16),
            pltpu.VMEM((2, tokens // 2, 2 * width), BF16),
            pltpu.VMEM((2, n_sp, 2, model), BF16),
            pltpu.VMEM((2, n_sp, 2, model), BF16),
            pltpu.VMEM((2 * n_sp, model), BF16),
            pltpu.VMEM((2 * n_sp, fe), BF16),
            pltpu.VMEM((2, n_sp, 2, model), BF16),
            pltpu.VMEM((2, n_sp, 2, model), BF16),
            dma((4,)), dma((3 * SIDE,)), dma((3 * SIDE,)), dma((2,)), dma((2,)), dma((2,)), dma((2,)),
            dma((2,)), dma((2,)), dma((SMALL,)),
        ],
        compiler_params=pltpu.CompilerParams(
            collective_id=0, has_side_effects=True, vmem_limit_bytes=60 * 1024 * 1024
        ),
        name="layer",
    )(*smalls, out_proj, gate_proj, up_proj, down_proj)
    return result


def solution(mesh):
    return jax.shard_map(
        local,
        mesh=mesh,
        in_specs=(
            P("sp", "tp"),
            P("sp", "tp"),
            P(None, None, "tp", None),
            P(None, None, "tp", None),
            P(None, None, "tp"),
            P(None, None, "tp", "sp"),
            P(None, None, "tp", None, None),
            P(None, None, "tp", None, None),
            P(None, None, "tp", None, None),
            P(None, None, "tp", None, None),
            P(None, "tp"),
            P(None, "tp", None, None),
            P(("sp", "tp"), None),
            P(),
            P(),
            P(),
            P(("sp", "tp"), None),
            P(("sp", "tp"), None),
            P(("sp", "tp"), None, None),
            P(("sp", "tp"), None, None),
            P(("sp", "tp"), None, None),
        ),
        out_specs=P(("sp", "tp"), None),
        check_vma=False,
    )
```
